32 devices in a mesh: grp: 2 (over y), sp: 4 (over z), tp: 4 (over x, core).
Axes of the slice: x: 2, y: 2, z: 4, core: 2. Of those that a mesh axis runs over, the one named last changes fastest.
Arguments:
- target: bfloat16 [1024, 2048], P(('grp', 'sp', 'tp')), parts along dimension 0, may hold values from -5 to 5
- source: bfloat16 [8192, 2048], P(('grp', 'sp', 'tp')), parts along dimension 0, may hold values from -5 to 5
- source_gain: float32 [2048], replicated, may hold values from 0.1 to 1.9
- pre_first: float32 [2048], replicated, may hold values from 0.1 to 1.9
- query_first: bfloat16 [2048, 2048], P(None, 'tp')
- keyval_first: bfloat16 [2048, 1024], P(None, 'tp')
- out_first: bfloat16 [2048, 2048], P('tp'), may hold values from -0.125 to 0.125
- post_first: float32 [2048], replicated, may hold values from 0.1 to 1.9
- ffn_pre: float32 [2048], replicated, may hold values from 0.1 to 1.9
- w_gate: bfloat16 [2048, 2816], P(None, 'tp'), may hold values from -0.125 to 0.125
- w_value: bfloat16 [2048, 2816], P(None, 'tp'), may hold values from -0.125 to 0.125
- conv_gate: float32 [3, 2816], P(None, 'tp'), may hold values from -3.5 to 3.5
- conv_value: float32 [3, 2816], P(None, 'tp'), may hold values from -3.5 to 3.5
- w_down: bfloat16 [2816, 2048], P('tp'), may hold values from -0.109375 to 0.109375
- ffn_post: float32 [2048], replicated, may hold values from 0.1 to 1.9
- pre_second: float32 [2048], replicated, may hold values from 0.1 to 1.9
- query_second: bfloat16 [2048, 2048], P(None, 'tp')
- keyval_second: bfloat16 [2048, 1024], P(None, 'tp')
- out_second: bfloat16 [2048, 2048], P('tp'), may hold values from -0.125 to 0.125
- post_second: float32 [2048], replicated, may hold values from 0.1 to 1.9
Outputs:
- decoded: float32 [1024, 2048], P(('grp', 'sp', 'tp')), parts along dimension 0
The draws below stay inside these ranges and needn't reach their ends.
There are 2 independent parts, one for each index of `grp`. The reference program is written for one: setup_inputs(seed, part) draws one part's arguments, and reference() takes and returns one part's arrays. A program takes and returns all parts, laid end to end along the dimension named above; an argument that names none is the same for every part. Nothing has to cross between parts.
All inputs are finite; a program needn't handle non-finite values.
Results may differ from the reference program's by a relative error of at most 0.04.
Values may be sent and summed in bfloat16 or wider, within the bound.
No kernel may reach another device: no remote copies, remote signals or barrier semaphores. Data moves between devices by JAX's collectives and lax.ppermute only.
A program may use at most 128 MiB of HBM per device.

```python
import jax
import jax.numpy as jnp
from jax import lax

D = 2048
HEAD = 128
QH = 16
KVH = 4
FF = 2816
TARGET = 512
SOURCE = 4096
N_TP = 4


def draw_target(key, part):
    rows = jnp.clip(jax.random.normal(jax.random.fold_in(key, 11), (TARGET, D), jnp.float32), -5.0, 5.0)
    return rows.astype(jnp.bfloat16)


def draw_source(key, part):
    rows = jnp.clip(jax.random.normal(jax.random.fold_in(key, 12), (SOURCE, D), jnp.float32), -5.0, 5.0)
    return rows.astype(jnp.bfloat16)


def layer_weights(key, salt):
    drawn_query = jax.random.normal(jax.random.fold_in(key, salt + 1), (D, QH * HEAD), jnp.float32) * D ** (-0.5)
    drawn_keyval = jax.random.normal(jax.random.fold_in(key, salt + 2), (D, KVH, 2, HEAD), jnp.float32) * D ** (-0.5)
    return (drawn_query, drawn_keyval.reshape(D, KVH * 2 * HEAD))


def draw_query_first(key, part):
    return layer_weights(key, 41)[0].astype(jnp.bfloat16)


def draw_keyval_first(key, part):
    return layer_weights(key, 41)[1].astype(jnp.bfloat16)


def draw_query_second(key, part):
    return layer_weights(key, 51)[0].astype(jnp.bfloat16)


def draw_keyval_second(key, part):
    return layer_weights(key, 51)[1].astype(jnp.bfloat16)


def block_levels(stream_key, dims, cuts, smallest, top_value):
    loudness, own = 1.0, jax.random.fold_in(stream_key, 6)
    for dim, shards_of in cuts:
        draws = jnp.exp(jax.random.uniform(jax.random.fold_in(own, dim), (shards_of,), jnp.float32, smallest / len(cuts), top_value / len(cuts)))
        loudness = loudness * jnp.repeat(draws, dims[dim] // shards_of).reshape([-1 if axis == dim else 1 for axis in range(len(dims))])
    return loudness


def bell_draw(own_key, shape, scale, bound, split=(), held_as=jnp.bfloat16):
    result = jax.random.normal(own_key, shape, jnp.float32) * scale
    if len(split) > 0:
        result = block_levels(own_key, shape, split, -0.22, 0.18) * result
    return jnp.clip(result, min=-bound, max=bound).astype(held_as)


def setup_inputs(seed: int = 0, part: int = 0) -> dict:
    key_of = jax.random.split(jax.random.key(seed), 21)
    part_splits = jax.random.split(jax.random.fold_in(key_of[20], part), 21)
    return {
        "target": draw_target(jax.random.fold_in(jax.random.fold_in(key_of[20], part), 71), part),
        "source": draw_source(jax.random.fold_in(jax.random.fold_in(key_of[20], part), 71), part),
        "source_gain": jnp.clip(jax.random.uniform(key_of[2], (D,), jnp.float32, 0.1, 1.9), 0.1, 1.9),
        "pre_first": jnp.clip(jax.random.uniform(key_of[3], (D,), jnp.float32, 0.1, 1.9), 0.1, 1.9),
        "query_first": draw_query_first(jax.random.fold_in(key_of[20], 71), part),
        "keyval_first": draw_keyval_first(jax.random.fold_in(key_of[20], 71), part),
        "out_first": bell_draw(key_of[6], (QH * HEAD, D), (QH * HEAD) ** -0.5, 0.125, ((0, 4),)),
        "post_first": jnp.clip(jax.random.uniform(key_of[7], (D,), jnp.float32, 0.1, 1.9), 0.1, 1.9),
        "ffn_pre": jnp.clip(jax.random.uniform(key_of[8], (D,), jnp.float32, 0.1, 1.9), 0.1, 1.9),
        "w_gate": bell_draw(key_of[9], (D, FF), D ** -0.5, 0.125, ((1, 4),)),
        "w_value": bell_draw(key_of[10], (D, FF), D ** -0.5, 0.125, ((1, 4),)),
        "conv_gate": bell_draw(key_of[11], (3, FF), 3 ** -0.5, 3.5, ((1, 4),), jnp.float32),
        "conv_value": bell_draw(key_of[12], (3, FF), 3 ** -0.5, 3.5, ((1, 4),), jnp.float32),
        "w_down": bell_draw(key_of[13], (FF, D), FF ** -0.5, 0.109375, ((0, 4),)),
        "ffn_post": jnp.clip(jax.random.uniform(key_of[14], (D,), jnp.float32, 0.1, 1.9), 0.1, 1.9),
        "pre_second": jnp.clip(jax.random.uniform(key_of[15], (D,), jnp.float32, 0.1, 1.9), 0.1, 1.9),
        "query_second": draw_query_second(jax.random.fold_in(key_of[20], 71), part),
        "keyval_second": draw_keyval_second(jax.random.fold_in(key_of[20], 71), part),
        "out_second": bell_draw(key_of[18], (QH * HEAD, D), (QH * HEAD) ** -0.5, 0.125, ((0, 4),)),
        "post_second": jnp.clip(jax.random.uniform(key_of[19], (D,), jnp.float32, 0.1, 1.9), 0.1, 1.9),
    }


def normed(values, gain):
    widened = values.astype(jnp.float32)
    return widened * lax.rsqrt(lax.optimization_barrier(jnp.mean(widened * widened, axis=-1, keepdims=True)) + 1e-06) * gain

def sharded_product(left_side, right_side, shards):
    column_span = left_side.shape[1] // shards

    def accumulate(running, shard_index):
        left_part = lax.dynamic_slice_in_dim(left_side, shard_index * column_span, column_span, 1)
        right_part = lax.dynamic_slice_in_dim(right_side, shard_index * column_span, column_span, 0)
        rounded = jnp.dot(left_part, right_part, preferred_element_type=jnp.float32).astype(jnp.bfloat16)
        rounded = lax.optimization_barrier(rounded)
        return (running + rounded.astype(jnp.float32), None)
    initial = jnp.zeros((left_side.shape[0], right_side.shape[1]), jnp.float32)
    summed, unused = lax.scan(accumulate, initial, jnp.arange(shards, dtype=jnp.int32))
    return summed

def attend(queries, keyvals):
    group_size = QH // KVH
    scale_factor = HEAD ** (-0.5)
    query_heads = jnp.moveaxis(queries.reshape(TARGET, QH, HEAD), 1, 0)

    def one_head(inputs):
        head_queries, head_index = inputs
        columns = lax.dynamic_slice_in_dim(keyvals, head_index // group_size * (2 * HEAD), 2 * HEAD, 1)
        head_keys = columns[:, :HEAD]
        head_values = columns[:, HEAD:]
        scores = lax.dot_general(head_queries, head_keys, (((1,), (1,)), ((), ())), preferred_element_type=jnp.float32) * scale_factor
        row_max = lax.optimization_barrier(jnp.max(scores, axis=1, keepdims=True))
        weights = jnp.exp(scores - row_max)
        weight_sum = lax.optimization_barrier(jnp.sum(weights, axis=1, keepdims=True))
        gathered = jnp.dot(weights.astype(jnp.bfloat16), head_values, preferred_element_type=jnp.float32)
        return (gathered / weight_sum).astype(jnp.bfloat16)
    outputs = lax.map(one_head, (query_heads, jnp.arange(QH, dtype=jnp.int32)))
    return jnp.moveaxis(outputs, 0, 1).reshape(TARGET, QH * HEAD)

def attention_layer(stream, pre_gain, w_query, keyvals, w_out, post_gain):
    hidden = normed(stream, pre_gain).astype(jnp.bfloat16)
    queries = jnp.dot(hidden, w_query, preferred_element_type=jnp.float32).astype(jnp.bfloat16)
    heads = attend(queries, keyvals)
    mixed = sharded_product(heads, w_out, N_TP)
    return stream.astype(jnp.float32) + normed(mixed, post_gain)

def causal_mix(up_rows, conv_taps):
    padded = jnp.pad(up_rows.astype(jnp.float32), ((2, 0), (0, 0)))
    length = up_rows.shape[0]
    return conv_taps[0] * padded[:length] + conv_taps[1] * padded[1:length + 1] + conv_taps[2] * padded[2:]

def reference(target, source, source_gain, pre_first, query_first, keyval_first, out_first, post_first, ffn_pre, w_gate, w_value, conv_gate, conv_value, w_down, ffn_post, pre_second, query_second, keyval_second, out_second, post_second):
    source_normed = normed(source, source_gain).astype(jnp.bfloat16)
    kv_first = jnp.dot(source_normed, keyval_first, preferred_element_type=jnp.float32).astype(jnp.bfloat16)
    kv_second = jnp.dot(source_normed, keyval_second, preferred_element_type=jnp.float32).astype(jnp.bfloat16)
    after_first = attention_layer(target, pre_first, query_first, kv_first, out_first, post_first)
    ffn_input = normed(after_first, ffn_pre).astype(jnp.bfloat16)
    up_gate = jnp.dot(ffn_input, w_gate, preferred_element_type=jnp.float32).astype(jnp.bfloat16)
    up_value = jnp.dot(ffn_input, w_value, preferred_element_type=jnp.float32).astype(jnp.bfloat16)
    gated = (jax.nn.gelu(causal_mix(up_gate, conv_gate), approximate=True) * causal_mix(up_value, conv_value)).astype(jnp.bfloat16)
    ffn_sum = sharded_product(gated, w_down, N_TP)
    after_ffn = after_first + normed(ffn_sum, ffn_post)
    return attention_layer(after_ffn, pre_second, query_second, kv_second, out_second, post_second)
```

```python
import functools

import jax
import jax.numpy as jnp
from jax import lax
from jax.experimental import pallas as pl
from jax.experimental.pallas import tpu as pltpu
from jax.sharding import PartitionSpec as P

HEAD = 128


def swapped(block, axis, distance):
    count = lax.axis_size(axis)
    route = []
    for low in range(count):
        high = low | 1 << distance
        if high != low and high < count:
            route += [(low, high), (high, low)]
    return lax.ppermute(block, axis, route)


def shifted(value, axis, steps):
    count = lax.axis_size(axis)
    leading, last = (max(0, -steps), min(count, count - steps))
    return lax.ppermute(value, axis, [(source, source + steps) for source in range(leading, last)])


def normed(values, gain):
    widened = values.astype(jnp.float32)
    return widened * lax.rsqrt(jnp.mean(widened * widened, axis=-1, keepdims=True) + 1e-06) * gain


def project_rows(rows_here, weights):
    shard_rows = lax.all_gather(rows_here, "tp", axis=0, tiled=True)
    products = [
        jnp.dot(shard_rows, weight, preferred_element_type=jnp.float32).astype(jnp.bfloat16)
        for weight in weights
    ]
    return jnp.concatenate(products, axis=1)


def summed_rows(parts, weight):
    return lax.psum_scatter(
        jnp.dot(parts, weight, preferred_element_type=jnp.float32).astype(jnp.bfloat16),
        "tp",
        scatter_dimension=0,
        tiled=True,
    ).astype(jnp.float32)


def key_columns(source_rows, keyval_first, keyval_second):
    both_layers = jnp.concatenate([keyval_first, keyval_second], axis=1)
    columns = jnp.einsum(
        "rd,dc->cr",
        lax.all_gather(source_rows, "tp", axis=0, tiled=True),
        both_layers,
        preferred_element_type=jnp.float32,
    ).astype(jnp.bfloat16)
    column_count = keyval_first.shape[1]
    stacked = columns.reshape(2, column_count, columns.shape[1])
    own_index = lax.axis_index("tp")
    doublings = (2 * HEAD // column_count).bit_length() - 1
    for bit_number in range(doublings):
        lower_half = own_index // 2**bit_number % 2 == 0
        outgoing = stacked
        retained = stacked
        partner = swapped(outgoing, "tp", bit_number)
        stacked = jnp.where(
            lower_half,
            jnp.concatenate([retained, partner], axis=1),
            jnp.concatenate([partner, retained], axis=1),
        )
    return (stacked[:, :HEAD], stacked[:, HEAD:])


def absorber(query_heads, running, shard_pair):
    scale_factor = HEAD ** (-0.5)
    best_score, weight_sum, weighted = running
    key_block, value_block = shard_pair
    scores = (
        jnp.einsum("thd,ds->ths", query_heads, key_block, preferred_element_type=jnp.float32)
        * scale_factor
    )
    newest = jnp.max(scores, axis=2)
    rescale = jnp.exp(best_score - newest)
    weights = jnp.exp(scores - newest[:, :, None])
    weight_sum = weight_sum * rescale + jnp.sum(weights, axis=2)
    weighted = weighted * rescale[:, :, None] + jnp.einsum(
        "ths,ds->thd", weights.astype(jnp.bfloat16), value_block, preferred_element_type=jnp.float32
    )
    return (newest, weight_sum, weighted)


def empty_running(row_count, head_count):
    return (
        jnp.full((row_count, head_count), -jnp.inf, jnp.float32),
        jnp.zeros((row_count, head_count), jnp.float32),
        jnp.zeros((row_count, head_count, HEAD), jnp.float32),
    )


def attend_keys(queries, keys_t, values_t):
    row_count = queries.shape[0]
    head_count = queries.shape[1] // HEAD
    query_heads = queries.reshape(row_count, head_count, HEAD)
    best_score, weight_sum, weighted = absorber(
        query_heads,
        empty_running(row_count, head_count),
        (
            lax.all_gather(keys_t, "sp", axis=1, tiled=True),
            lax.all_gather(values_t, "sp", axis=1, tiled=True),
        ),
    )
    return (
        (weighted / weight_sum[:, :, None])
        .reshape(row_count, head_count * HEAD)
        .astype(jnp.bfloat16)
    )


def causal_mix(rim_rows, up_rows, conv_taps):
    padded = jnp.concatenate([rim_rows, up_rows], axis=0).astype(jnp.float32)
    length = up_rows.shape[0]
    return (
        conv_taps[0] * padded[:length]
        + conv_taps[1] * padded[1 : length + 1]
        + conv_taps[2] * padded[2:]
    )


def per_device(
    target,
    source,
    source_gain,
    pre_first,
    query_first,
    keyval_first,
    out_first,
    post_first,
    ffn_pre,
    w_gate,
    w_value,
    conv_gate,
    conv_value,
    w_down,
    ffn_post,
    pre_second,
    query_second,
    keyval_second,
    out_second,
    post_second,
):
    source_rows = normed(source, source_gain).astype(jnp.bfloat16)
    keys_t, values_t = key_columns(source_rows, keyval_first, keyval_second)

    def attention_layer(stream, pre_gain, w_query, layer_index, w_out, post_gain):
        queries = project_rows(normed(stream, pre_gain).astype(jnp.bfloat16), (w_query,))
        heads = attend_keys(queries, keys_t[layer_index], values_t[layer_index])
        mixed = summed_rows(heads, w_out)
        return stream.astype(jnp.float32) + normed(mixed, post_gain)

    after_first = attention_layer(target, pre_first, query_first, 0, out_first, post_first)
    up_both = project_rows(normed(after_first, ffn_pre).astype(jnp.bfloat16), (w_gate, w_value))
    hidden_width = w_gate.shape[1]
    up_gate = up_both[:, :hidden_width]
    up_value = up_both[:, hidden_width:]
    rim_gate, rim_value = shifted((up_gate[-2:], up_value[-2:]), "sp", 1)
    gated = (
        jax.nn.gelu(causal_mix(rim_gate, up_gate, conv_gate), approximate=True)
        * causal_mix(rim_value, up_value, conv_value)
    ).astype(jnp.bfloat16)
    ffn_sum = summed_rows(gated, w_down)
    after_ffn = after_first + normed(ffn_sum, ffn_post)
    return attention_layer(after_ffn, pre_second, query_second, 1, out_second, post_second)


def swapped_mask(block, axis, mask):
    count = lax.axis_size(axis)
    return lax.ppermute(block, axis, [(index, index ^ mask) for index in range(count)])


def launch(body, outs, *operands, scratch=(), limit=24):
    return pl.pallas_call(
        body,
        out_shape=outs,
        scratch_shapes=list(scratch),
        compiler_params=pltpu.CompilerParams(vmem_limit_bytes=limit << 20),
    )(*operands)


def dot32(left, right):
    return jnp.dot(left, right, preferred_element_type=jnp.float32)


def dot_nt(left, right):
    return lax.dot_general(
        left, right, (((1,), (1,)), ((), ())), preferred_element_type=jnp.float32
    )


def query_body(top_ref, low_ref, gain_ref, weight_ref, out_ref):
    half = top_ref.shape[0]
    for index, ref in enumerate((top_ref, low_ref)):
        hidden = normed(ref[...], gain_ref[...]).astype(jnp.bfloat16)
        out_ref[index * half : (index + 1) * half] = dot32(hidden, weight_ref[...]).astype(
            jnp.bfloat16
        )


def keyval_body(*refs):
    *row_refs, gain_ref, weight_ref, rows_out, keyval_out = refs
    start = 0
    for ref in row_refs:
        stop = start + ref.shape[0]
        rows_out[start:stop] = normed(ref[...], gain_ref[...]).astype(jnp.bfloat16)
        start = stop
    keyval_out[...] = dot32(rows_out[...], weight_ref[...]).astype(jnp.bfloat16)


def project_body(*refs):
    *row_refs, weight_ref, out_ref = refs
    start = 0
    for ref in row_refs:
        stop = start + ref.shape[0]
        out_ref[start:stop] = dot32(ref[...], weight_ref[...]).astype(jnp.bfloat16)
        start = stop


EXPONENT_SCALE = HEAD ** (-0.5) * 1.4426950408889634


def head_partial(query, keyval_refs):
    scores = [dot_nt(query, ref[:, :HEAD]) for ref in keyval_refs]
    best = functools.reduce(
        jnp.maximum, [jnp.max(block, axis=1, keepdims=True) for block in scores]
    )
    weight_sum, weighted = 0.0, 0.0
    for block, ref in zip(scores, keyval_refs):
        weights = jnp.exp2((block - best) * EXPONENT_SCALE)
        weight_sum += jnp.sum(weights, axis=1, keepdims=True)
        weighted += dot32(weights.astype(jnp.bfloat16), ref[:, HEAD:])
    return best, weight_sum, weighted


STAT_ROWS = 16


def partial_body(query_ref, *refs):
    *keyval_refs, out_ref = refs
    rows, width = query_ref.shape
    lane = lax.broadcasted_iota(jnp.int32, (rows, HEAD), 1)
    levels = jnp.zeros((rows, HEAD), jnp.float32)
    for head in range(width // HEAD):
        columns = slice(head * HEAD, (head + 1) * HEAD)
        best, weight_sum, weighted = head_partial(query_ref[:, columns], keyval_refs)
        out_ref[:rows, columns] = (weighted / weight_sum).astype(jnp.bfloat16)
        level = best * EXPONENT_SCALE + jnp.log2(weight_sum)
        levels = jnp.where(lane == head, level, levels)
    left = levels.T[:STAT_ROWS]
    for piece in range(3):
        rounded = left.astype(jnp.bfloat16)
        out_ref[rows:, piece * rows : (piece + 1) * rows] = rounded
        left = left - rounded.astype(jnp.float32)


def joined_heads(partial_refs, heads_ref):
    rows, width = heads_ref.shape
    levels = [
        sum(
            ref[rows:, piece * rows : (piece + 1) * rows].astype(jnp.float32) for piece in range(3)
        )
        for ref in partial_refs
    ]
    best = functools.reduce(jnp.maximum, levels)
    shares = [jnp.exp2(level - best) for level in levels]
    total = functools.reduce(jnp.add, shares)
    filler = jnp.zeros((HEAD - STAT_ROWS, rows), jnp.float32)
    columns = [jnp.concatenate([share / total, filler], axis=0).T for share in shares]
    for head in range(width // HEAD):
        part = slice(head * HEAD, (head + 1) * HEAD)
        heads_ref[:, part] = sum(
            ref[:rows, part].astype(jnp.float32) * column[:, head : head + 1]
            for ref, column in zip(partial_refs, columns)
        ).astype(jnp.bfloat16)


def join_out_body(*refs):
    *partial_refs, weight_ref, keep_ref, send_ref, heads_ref = refs
    joined_heads(partial_refs, heads_ref)
    half = keep_ref.shape[0]
    send_ref[...] = dot32(heads_ref[half:], weight_ref[...]).astype(jnp.bfloat16)
    keep_ref[...] = dot32(heads_ref[:half], weight_ref[...]).astype(jnp.bfloat16)


def residual_body(own_ref, other_ref, stream_ref, post_ref, pre_ref, stream_out, hidden_out):
    quarter = own_ref.shape[0] // 2
    for index in range(2):
        here = slice(index * quarter, (index + 1) * quarter)
        there = slice((1 - index) * quarter, (2 - index) * quarter)
        mixed = own_ref[here].astype(jnp.float32) + other_ref[there].astype(jnp.float32)
        stream = stream_ref[here].astype(jnp.float32) + normed(mixed, post_ref[...])
        stream_out[here] = stream
        hidden_out[here] = normed(stream, pre_ref[...]).astype(jnp.bfloat16)


def last_body(own_ref, other_ref, stream_ref, post_ref, out_ref):
    mixed = own_ref[...].astype(jnp.float32) + other_ref[...].astype(jnp.float32)
    out_ref[...] = stream_ref[...] + normed(mixed, post_ref[...])


LOCAL_ORDER = (0, 2, 1, 3)


def up_body(own_ref, other_ref, gate_ref, value_ref, gate_out, value_out):
    quarter = own_ref.shape[0] // 2
    place = lax.axis_index("tp")
    rows = jnp.concatenate([own_ref[...], other_ref[...]], axis=0)
    for weight_ref, out_ref in ((gate_ref, gate_out), (value_ref, value_out)):
        product = dot32(rows, weight_ref[...]).astype(jnp.bfloat16)
        for index, mask in enumerate(LOCAL_ORDER):
            where = pl.multiple_of((place ^ mask) * quarter, quarter)
            out_ref[pl.ds(where, quarter)] = product[index * quarter : (index + 1) * quarter]


def mixed_taps(rim_ref, up_ref, taps_ref):
    ups = jnp.concatenate(
        [rim_ref[...].astype(jnp.float32), up_ref[...].astype(jnp.float32)], axis=0
    )
    rim, rows = rim_ref.shape[0], up_ref.shape[0]
    return sum(
        taps_ref[tap : tap + 1] * ups[rim - 2 + tap : rim - 2 + tap + rows] for tap in range(3)
    )


def down_body(
    rim_gate, up_gate, conv_gate, rim_value, up_value, conv_value, down_ref, keep_ref, send_ref, gated_ref
):
    gated_ref[...] = (
        jax.nn.gelu(mixed_taps(rim_gate, up_gate, conv_gate), approximate=True)
        * mixed_taps(rim_value, up_value, conv_value)
    ).astype(jnp.bfloat16)
    quarter = keep_ref.shape[0] // 2
    place = lax.axis_index("tp")
    for ref, masks in ((send_ref, LOCAL_ORDER[2:]), (keep_ref, LOCAL_ORDER[:2])):
        rows = jnp.concatenate(
            [
                gated_ref[pl.ds(pl.multiple_of((place ^ mask) * quarter, quarter), quarter)]
                for mask in masks
            ],
            axis=0,
        )
        ref[...] = dot32(rows, down_ref[...]).astype(jnp.bfloat16)


def second_body(*refs):
    own_ref, other_ref, query_ref, *keyval_refs, weight_ref, keep_ref, send_ref, queries_ref, heads_ref = refs
    half = own_ref.shape[0]
    queries_ref[:half] = dot32(own_ref[...], query_ref[...]).astype(jnp.bfloat16)
    queries_ref[half:] = dot32(other_ref[...], query_ref[...]).astype(jnp.bfloat16)
    for head in range(heads_ref.shape[1] // HEAD):
        columns = slice(head * HEAD, (head + 1) * HEAD)
        best, weight_sum, weighted = head_partial(queries_ref[:, columns], keyval_refs)
        heads_ref[:, columns] = (weighted / weight_sum).astype(jnp.bfloat16)
    send_ref[...] = dot32(heads_ref[half:], weight_ref[...]).astype(jnp.bfloat16)
    keep_ref[...] = dot32(heads_ref[:half], weight_ref[...]).astype(jnp.bfloat16)


def shape_of(rows, columns, dtype=jnp.bfloat16):
    return jax.ShapeDtypeStruct((rows, columns), dtype)


CHUNKS = 4


def per_device_paired(
    target,
    source,
    source_gain,
    pre_first,
    query_first,
    keyval_first,
    out_first,
    post_first,
    ffn_pre,
    w_gate,
    w_value,
    conv_gate,
    conv_value,
    w_down,
    ffn_post,
    pre_second,
    query_second,
    keyval_second,
    out_second,
    post_second,
):
    quarter, width = target.shape
    half, rows = 2 * quarter, 4 * quarter
    head_width, keyval_width, hidden_width = query_first.shape[1], keyval_first.shape[1], w_gate.shape[1]
    sp_count = lax.axis_size("sp")
    row = lambda gain: gain.reshape(1, -1)

    own_target = jnp.concatenate([target, swapped_mask(target, "tp", 2)], axis=0)
    other_target = swapped_mask(own_target, "tp", 1)
    queries = launch(
        query_body, shape_of(rows, head_width), own_target, other_target, row(pre_first), query_first
    )
    query_blocks = [queries] + [swapped_mask(queries, "sp", mask) for mask in range(1, sp_count)]

    span = source.shape[0] // CHUNKS
    normed_rows, keyvals_first = [], []
    for chunk in range(CHUNKS):
        here = source[chunk * span : (chunk + 1) * span]
        across = swapped_mask(here, "tp", 2)
        pieces = (here, swapped_mask(here, "tp", 1), across, swapped_mask(across, "tp", 1))
        chunk_rows, chunk_keyval = launch(
            keyval_body,
            (shape_of(4 * span, width), shape_of(4 * span, keyval_width)),
            *pieces,
            row(source_gain),
            keyval_first,
        )
        normed_rows.append(chunk_rows)
        keyvals_first.append(chunk_keyval)
    keyval_here = launch(
        project_body, shape_of(4 * source.shape[0], keyval_width), *normed_rows, keyval_second
    )

    packed = shape_of(rows + STAT_ROWS, head_width)
    partials = [None] * sp_count
    for mask in (3, 2, 1, 0) if sp_count == 4 else range(sp_count - 1, -1, -1):
        partial = launch(partial_body, packed, query_blocks[mask], *keyvals_first)
        partials[mask] = swapped_mask(partial, "sp", mask) if mask else partial
    halves = (shape_of(half, width), shape_of(half, width))

    def pair_sum(keep, send):
        received = swapped_mask(send, "tp", 1)
        return (keep.astype(jnp.float32) + received.astype(jnp.float32)).astype(jnp.bfloat16)

    def residual(own, stream, post_gain, pre_gain):
        other = swapped_mask(own, "tp", 2)
        stream, hidden = launch(
            residual_body,
            (shape_of(half, width, jnp.float32), shape_of(half, width)),
            own,
            other,
            stream,
            row(post_gain),
            row(pre_gain),
        )
        return stream, hidden, swapped_mask(hidden, "tp", 1)

    keep, send = launch(
        join_out_body,
        halves,
        *partials,
        out_first,
        scratch=[pltpu.VMEM((rows, head_width), jnp.bfloat16)],
    )
    own = pair_sum(keep, send)

    keyval_here, own = lax.optimization_barrier((keyval_here, own))
    keyvals_second = [keyval_here]
    for bit in reversed(range((sp_count - 1).bit_length())):
        keyvals_second += [swapped_mask(part, "sp", 1 << bit) for part in keyvals_second]

    after_first, hidden, other_hidden = residual(own, own_target, post_first, ffn_pre)
    up_gate, up_value = launch(
        up_body,
        (shape_of(rows, hidden_width), shape_of(rows, hidden_width)),
        hidden,
        other_hidden,
        w_gate,
        w_value,
    )
    rim = jnp.concatenate([up_gate[-8:], up_value[-8:]], axis=0)
    rim = shifted(rim, "sp", 1)
    keep, send = launch(
        down_body,
        halves,
        rim[:8],
        up_gate,
        conv_gate,
        rim[8:],
        up_value,
        conv_value,
        w_down,
        scratch=[pltpu.VMEM((rows, hidden_width), jnp.bfloat16)],
    )
    after_ffn, hidden, other_hidden = residual(pair_sum(keep, send), after_first, ffn_post, pre_second)
    keep, send = launch(
        second_body,
        halves,
        hidden,
        other_hidden,
        query_second,
        *keyvals_second,
        out_second,
        scratch=[pltpu.VMEM((rows, head_width), jnp.bfloat16)] * 2,
        limit=32,
    )
    own = pair_sum(keep, send)
    return launch(
        last_body,
        shape_of(quarter, width, jnp.float32),
        own[:quarter],
        swapped_mask(own[quarter:], "tp", 2),
        after_ffn[:quarter],
        row(post_second),
    )


def chosen(*arrays):
    target, keyval_first, query_first = arrays[0], arrays[5], arrays[4]
    sp_count = lax.axis_size("sp")
    fits = (
        lax.axis_size("tp") == 4
        and sp_count & (sp_count - 1) == 0
        and 4 * target.shape[0] == HEAD
        and keyval_first.shape[1] == 2 * HEAD
        and 3 * HEAD <= query_first.shape[1] <= STAT_ROWS * HEAD
    )
    return (per_device_paired if fits else per_device)(*arrays)


def solution(mesh):
    placed = (
        P(("grp", "sp", "tp"), None),
        P(("grp", "sp", "tp"), None),
        P(),
        P(),
        P(None, "tp"),
        P(None, "tp"),
        P("tp", None),
        P(),
        P(),
        P(None, "tp"),
        P(None, "tp"),
        P(None, "tp"),
        P(None, "tp"),
        P("tp", None),
        P(),
        P(),
        P(None, "tp"),
        P(None, "tp"),
        P("tp", None),
        P(),
    )
    return jax.shard_map(
        chosen,
        mesh=mesh,
        in_specs=placed,
        out_specs=P(("grp", "sp", "tp"), None),
        check_vma=False,
    )
```

```python
import functools

import jax
import jax.numpy as jnp
from jax import lax
from jax.experimental import pallas as pl
from jax.experimental.pallas import tpu as pltpu
from jax.sharding import PartitionSpec as P


HEAD = 128


def swapped(block, axis, distance):
    count = lax.axis_size(axis)
    route = []
    for low in range(count):
        high = low | 1 << distance
        if high != low and high < count:
            route += [(low, high), (high, low)]
    return lax.ppermute(block, axis, route)


def shifted(value, axis, steps):
    count = lax.axis_size(axis)
    leading, last = (max(0, -steps), min(count, count - steps))
    return lax.ppermute(value, axis, [(source, source + steps) for source in range(leading, last)])


def normed(values, gain):
    widened = values.astype(jnp.float32)
    return widened * lax.rsqrt(jnp.mean(widened * widened, axis=-1, keepdims=True) + 1e-06) * gain


def project_rows(rows_here, weights):
    shard_rows = lax.all_gather(rows_here, "tp", axis=0, tiled=True)
    products = [
        jnp.dot(shard_rows, weight, preferred_element_type=jnp.float32).astype(jnp.bfloat16)
        for weight in weights
    ]
    return jnp.concatenate(products, axis=1)


def summed_rows(parts, weight):
    return lax.psum_scatter(
        jnp.dot(parts, weight, preferred_element_type=jnp.float32).astype(jnp.bfloat16),
        "tp",
        scatter_dimension=0,
        tiled=True,
    ).astype(jnp.float32)


def key_columns(source_rows, keyval_first, keyval_second):
    both_layers = jnp.concatenate([keyval_first, keyval_second], axis=1)
    columns = jnp.einsum(
        "rd,dc->cr",
        lax.all_gather(source_rows, "tp", axis=0, tiled=True),
        both_layers,
        preferred_element_type=jnp.float32,
    ).astype(jnp.bfloat16)
    column_count = keyval_first.shape[1]
    stacked = columns.reshape(2, column_count, columns.shape[1])
    own_index = lax.axis_index("tp")
    doublings = (2 * HEAD // column_count).bit_length() - 1
    for bit_number in range(doublings):
        lower_half = own_index // 2**bit_number % 2 == 0
        outgoing = stacked
        retained = stacked
        partner = swapped(outgoing, "tp", bit_number)
        stacked = jnp.where(
            lower_half,
            jnp.concatenate([retained, partner], axis=1),
            jnp.concatenate([partner, retained], axis=1),
        )
    return (stacked[:, :HEAD], stacked[:, HEAD:])


def absorber(query_heads, running, shard_pair):
    scale_factor = HEAD ** (-0.5)
    best_score, weight_sum, weighted = running
    key_block, value_block = shard_pair
    scores = (
        jnp.einsum("thd,ds->ths", query_heads, key_block, preferred_element_type=jnp.float32)
        * scale_factor
    )
    newest = jnp.max(scores, axis=2)
    rescale = jnp.exp(best_score - newest)
    weights = jnp.exp(scores - newest[:, :, None])
    weight_sum = weight_sum * rescale + jnp.sum(weights, axis=2)
    weighted = weighted * rescale[:, :, None] + jnp.einsum(
        "ths,ds->thd", weights.astype(jnp.bfloat16), value_block, preferred_element_type=jnp.float32
    )
    return (newest, weight_sum, weighted)


def empty_running(row_count, head_count):
    return (
        jnp.full((row_count, head_count), -jnp.inf, jnp.float32),
        jnp.zeros((row_count, head_count), jnp.float32),
        jnp.zeros((row_count, head_count, HEAD), jnp.float32),
    )


def attend_keys(queries, keys_t, values_t):
    row_count = queries.shape[0]
    head_count = queries.shape[1] // HEAD
    query_heads = queries.reshape(row_count, head_count, HEAD)
    _, weight_sum, weighted = absorber(
        query_heads,
        empty_running(row_count, head_count),
        (
            lax.all_gather(keys_t, "sp", axis=1, tiled=True),
            lax.all_gather(values_t, "sp", axis=1, tiled=True),
        ),
    )
    return (
        (weighted / weight_sum[:, :, None])
        .reshape(row_count, head_count * HEAD)
        .astype(jnp.bfloat16)
    )


def causal_mix(rim_rows, up_rows, conv_taps):
    padded = jnp.concatenate([rim_rows, up_rows], axis=0).astype(jnp.float32)
    length = up_rows.shape[0]
    return (
        conv_taps[0] * padded[:length]
        + conv_taps[1] * padded[1 : length + 1]
        + conv_taps[2] * padded[2:]
    )


def per_device(
    target,
    source,
    source_gain,
    pre_first,
    query_first,
    keyval_first,
    out_first,
    post_first,
    ffn_pre,
    w_gate,
    w_value,
    conv_gate,
    conv_value,
    w_down,
    ffn_post,
    pre_second,
    query_second,
    keyval_second,
    out_second,
    post_second,
):
    source_rows = normed(source, source_gain).astype(jnp.bfloat16)
    keys_t, values_t = key_columns(source_rows, keyval_first, keyval_second)

    def attention_layer(stream, pre_gain, w_query, layer_index, w_out, post_gain):
        queries = project_rows(normed(stream, pre_gain).astype(jnp.bfloat16), (w_query,))
        heads = attend_keys(queries, keys_t[layer_index], values_t[layer_index])
        mixed = summed_rows(heads, w_out)
        return stream.astype(jnp.float32) + normed(mixed, post_gain)

    after_first = attention_layer(target, pre_first, query_first, 0, out_first, post_first)
    up_both = project_rows(normed(after_first, ffn_pre).astype(jnp.bfloat16), (w_gate, w_value))
    hidden_width = w_gate.shape[1]
    up_gate = up_both[:, :hidden_width]
    up_value = up_both[:, hidden_width:]
    rim_gate, rim_value = shifted((up_gate[-2:], up_value[-2:]), "sp", 1)
    gated = (
        jax.nn.gelu(causal_mix(rim_gate, up_gate, conv_gate), approximate=True)
        * causal_mix(rim_value, up_value, conv_value)
    ).astype(jnp.bfloat16)
    ffn_sum = summed_rows(gated, w_down)
    after_ffn = after_first + normed(ffn_sum, ffn_post)
    return attention_layer(after_ffn, pre_second, query_second, 1, out_second, post_second)


def swapped_mask(block, axis, mask):
    count = lax.axis_size(axis)
    return lax.ppermute(block, axis, [(index, index ^ mask) for index in range(count)])


def launch(body, outs, *operands, scratch=(), limit=24):
    return pl.pallas_call(
        body,
        out_shape=outs,
        scratch_shapes=list(scratch),
        compiler_params=pltpu.CompilerParams(vmem_limit_bytes=limit << 20),
    )(*operands)


def dot32(left, right):
    return jnp.dot(left, right, preferred_element_type=jnp.float32)


def dot_nt(left, right):
    return lax.dot_general(
        left, right, (((1,), (1,)), ((), ())), preferred_element_type=jnp.float32
    )


LOCAL_ORDER = (0, 2, 1, 3)
RIM_ROWS = 8


def last_quarter():
    mask = lax.axis_index("tp") ^ 3
    return (mask >> 1) + (mask & 1) * 2


def tail_rows(ref, quarter):
    start = pl.multiple_of((last_quarter() + 1) * quarter - 2 * RIM_ROWS, 2 * RIM_ROWS)
    return ref[pl.ds(start, 2 * RIM_ROWS)][RIM_ROWS:]


def query_body(own_ref, other_ref, gain_ref, weight_ref, out_ref, tail_ref, rows_ref):
    half = own_ref.shape[0]
    for index, ref in enumerate((own_ref, other_ref)):
        here = slice(index * half, (index + 1) * half)
        rows_ref[here] = ref[...]
        hidden = normed(ref[...], gain_ref[...]).astype(jnp.bfloat16)
        out_ref[here] = dot32(hidden, weight_ref[...]).astype(jnp.bfloat16)
    tail_ref[...] = tail_rows(rows_ref, half // 2)


def keyval_body(cut, here_ref, beside_ref, *refs):
    *row_refs, gain_ref, weight_ref, rows_out, keyval_out = refs
    start = 0
    for rows in [ref[cut] for ref in (here_ref, beside_ref)] + [ref[...] for ref in row_refs]:
        stop = start + rows.shape[0]
        rows_out[start:stop] = normed(rows, gain_ref[...]).astype(jnp.bfloat16)
        start = stop
    keyval_out[...] = dot32(rows_out[...], weight_ref[...]).astype(jnp.bfloat16)


def project_body(*refs):
    *row_refs, weight_ref, out_ref = refs
    start = 0
    for ref in row_refs:
        stop = start + ref.shape[0]
        out_ref[start:stop] = dot32(ref[...], weight_ref[...]).astype(jnp.bfloat16)
        start = stop


EXPONENT_SCALE = HEAD ** (-0.5) * 1.4426950408889634


def head_partial(query, keyval_refs):
    best = weighted = None
    for ref in keyval_refs:
        scores = dot_nt(query, ref[:, :HEAD]) * EXPONENT_SCALE
        newest = jnp.max(scores, axis=1, keepdims=True)
        if best is not None:
            newest = jnp.maximum(best, newest)
        weights = jnp.exp2(scores - newest).astype(jnp.bfloat16)
        ones = jnp.ones((ref.shape[0], HEAD), jnp.bfloat16)
        added = dot32(weights, jnp.concatenate([ref[:, HEAD:], ones], axis=1))
        weighted = added if best is None else weighted * jnp.exp2(best - newest) + added
        best = newest
    return best, weighted[:, HEAD:], weighted[:, :HEAD]


STAT_ROWS = 8
STAT_LANES = 32


def partial_body(mask, blocks, *refs):
    query_refs, keyval_refs, out_ref = refs[:blocks], refs[blocks:-1], refs[-1]
    rows, width = query_refs[0].shape
    block = lax.axis_index("sp")
    before = ((block ^ mask) - 1) ^ block
    rim = jnp.zeros((RIM_ROWS, width), jnp.bfloat16)
    for index, ref in enumerate(query_refs):
        rim = jnp.where(before == index, tail_rows(ref, rows // 4), rim)
    lane = lax.broadcasted_iota(jnp.int32, (rows + RIM_ROWS, HEAD), 1)
    levels = jnp.zeros((rows + RIM_ROWS, HEAD), jnp.float32)
    for head in range(width // HEAD):
        columns = slice(head * HEAD, (head + 1) * HEAD)
        query = jnp.concatenate([query_refs[mask][:, columns], rim[:, columns]], axis=0)
        best, weight_sum, weighted = head_partial(query, keyval_refs)
        out_ref[: rows + RIM_ROWS, columns] = (weighted / weight_sum).astype(jnp.bfloat16)
        levels = jnp.where(lane == head, best + jnp.log2(weight_sum), levels)
    left, rim_left = levels[:rows].T[:STAT_ROWS], levels[rows:, :STAT_LANES]
    for piece in range(3):
        for part, place, size in ((left, piece * rows, rows), (rim_left, 3 * rows + piece * STAT_LANES, STAT_LANES)):
            out_ref[rows + RIM_ROWS :, place : place + size] = part.astype(jnp.bfloat16)
        left = left - left.astype(jnp.bfloat16).astype(jnp.float32)
        rim_left = rim_left - rim_left.astype(jnp.bfloat16).astype(jnp.float32)


def shares_of(levels):
    best = functools.reduce(jnp.maximum, levels)
    shares = [jnp.exp2(level - best) for level in levels]
    total = functools.reduce(jnp.add, shares)
    return [share / total for share in shares]


def joined_heads(partial_refs, heads_ref):
    width = heads_ref.shape[1]
    rows = heads_ref.shape[0] - RIM_ROWS

    def levels(start, size):
        return [
            sum(
                ref[rows + RIM_ROWS :, start + piece * size : start + (piece + 1) * size].astype(jnp.float32)
                for piece in range(3)
            )
            for ref in partial_refs
        ]

    filler = jnp.zeros((HEAD - STAT_ROWS, rows), jnp.float32)
    columns = [
        jnp.concatenate([share, filler], axis=0).T for share in shares_of(levels(0, rows))
    ]
    for cut, parts in (
        (slice(0, rows), columns),
        (slice(rows, rows + RIM_ROWS), shares_of(levels(3 * rows, STAT_LANES))),
    ):
        for head in range(width // HEAD):
            lanes = slice(head * HEAD, (head + 1) * HEAD)
            heads_ref[cut, lanes] = sum(
                ref[cut, lanes].astype(jnp.float32) * part[:, head : head + 1]
                for ref, part in zip(partial_refs, parts)
            ).astype(jnp.bfloat16)


def join_send_body(*refs):
    *partial_refs, weight_ref, send_ref, heads_out, heads_ref = refs
    joined_heads(partial_refs, heads_ref)
    half = (heads_ref.shape[0] - RIM_ROWS) // 2
    send_ref[...] = dot32(heads_ref[half:], weight_ref[...]).astype(jnp.bfloat16)
    heads_out[:half] = heads_ref[:half]
    heads_out[half:] = heads_ref[2 * half :]


def residual_body(own_ref, other_ref, *refs):
    stream_ref, post_ref, pre_ref, stream_out, hidden_out = refs
    half = stream_out.shape[0]
    quarter = half // 2
    for index in range(2):
        here = slice(index * quarter, (index + 1) * quarter)
        there = slice((1 - index) * quarter, (2 - index) * quarter)
        mixed = own_ref[here].astype(jnp.float32) + other_ref[there].astype(jnp.float32)
        stream = stream_ref[here].astype(jnp.float32) + normed(mixed, post_ref[...])
        stream_out[here] = stream
        hidden_out[here] = normed(stream, pre_ref[...]).astype(jnp.bfloat16)


def residual_rim_body(own_ref, other_ref, stream_ref, rim_ref, post_ref, pre_ref, stream_out, hidden_out, rim_out):
    residual_body(own_ref, other_ref, stream_ref, post_ref, pre_ref, stream_out, hidden_out)
    half = stream_out.shape[0]
    mixed = own_ref[half:].astype(jnp.float32) + other_ref[half:].astype(jnp.float32)
    stream = rim_ref[...].astype(jnp.float32) + normed(mixed, post_ref[...])
    rim = normed(stream, pre_ref[...])
    rim_out[...] = jnp.where(lax.axis_index("sp") == 0, 0.0, rim).astype(jnp.bfloat16)


def last_body(own_ref, other_ref, stream_ref, post_ref, out_ref):
    mixed = own_ref[...].astype(jnp.float32) + other_ref[...].astype(jnp.float32)
    out_ref[...] = stream_ref[...] + normed(mixed, post_ref[...])


def mixed_taps(ups, taps_ref):
    rows = ups.shape[0] - RIM_ROWS
    return sum(
        taps_ref[tap : tap + 1] * ups[RIM_ROWS - 2 + tap : RIM_ROWS - 2 + tap + rows].astype(jnp.float32)
        for tap in range(3)
    )


def mixer_body(
    own_ref,
    other_ref,
    rim_ref,
    gate_ref,
    value_ref,
    conv_gate,
    conv_value,
    down_ref,
    send_ref,
    gated_out,
    ups_gate,
    ups_value,
    gated_ref,
):
    quarter = own_ref.shape[0] // 2
    place = lax.axis_index("tp")
    starts = [pl.multiple_of((place ^ mask) * quarter, quarter) for mask in LOCAL_ORDER]
    rows = jnp.concatenate([own_ref[...], other_ref[...], rim_ref[...]], axis=0)
    for weight_ref, ups in ((gate_ref, ups_gate), (value_ref, ups_value)):
        product = dot_nt(rows, weight_ref[...])
        ups[:RIM_ROWS] = product[4 * quarter :].astype(jnp.bfloat16).astype(jnp.float32)
        for index, start in enumerate(starts):
            ups[pl.ds(start + RIM_ROWS, quarter)] = (
                product[index * quarter : (index + 1) * quarter].astype(jnp.bfloat16).astype(jnp.float32)
            )
    gated_ref[...] = (
        jax.nn.gelu(mixed_taps(ups_gate[...], conv_gate), approximate=True)
        * mixed_taps(ups_value[...], conv_value)
    ).astype(jnp.bfloat16)
    parts = [gated_ref[pl.ds(start, quarter)] for start in starts]
    send_ref[...] = dot32(jnp.concatenate(parts[2:], axis=0), down_ref[...]).astype(jnp.bfloat16)
    gated_out[...] = jnp.concatenate(parts[:2], axis=0)


def second_body(*refs):
    own_ref, other_ref, query_ref, *keyval_refs, weight_ref, send_ref, heads_out, queries_ref, heads_ref = refs
    half = own_ref.shape[0]
    queries_ref[:half] = dot32(own_ref[...], query_ref[...]).astype(jnp.bfloat16)
    queries_ref[half:] = dot32(other_ref[...], query_ref[...]).astype(jnp.bfloat16)
    for head in range(heads_ref.shape[1] // HEAD):
        columns = slice(head * HEAD, (head + 1) * HEAD)
        _, weight_sum, weighted = head_partial(queries_ref[:, columns], keyval_refs)
        heads_ref[:, columns] = (weighted / weight_sum).astype(jnp.bfloat16)
    send_ref[...] = dot32(heads_ref[half:], weight_ref[...]).astype(jnp.bfloat16)
    heads_out[...] = heads_ref[:half]


def shape_of(rows, columns, dtype=jnp.bfloat16):
    return jax.ShapeDtypeStruct((rows, columns), dtype)


CHUNKS = 2


def per_device_paired(
    target,
    source,
    source_gain,
    pre_first,
    query_first,
    keyval_first,
    out_first,
    post_first,
    ffn_pre,
    w_gate,
    w_value,
    conv_gate,
    conv_value,
    w_down,
    ffn_post,
    pre_second,
    query_second,
    keyval_second,
    out_second,
    post_second,
):
    quarter, width = target.shape
    half, rows = 2 * quarter, 4 * quarter
    head_width, keyval_width, hidden_width = query_first.shape[1], keyval_first.shape[1], w_gate.shape[1]
    sp_count = lax.axis_size("sp")
    row = lambda gain: gain.reshape(1, -1)
    swap = lambda value, axis, mask: swapped_mask(value, axis, mask)
    wide = shape_of(half, width)

    own_target = jnp.concatenate([target, swap(target, "tp", 2)], axis=0)
    other_target = swap(own_target, "tp", 1)
    queries, tail = launch(
        query_body,
        (shape_of(rows, head_width), shape_of(RIM_ROWS, width)),
        own_target,
        other_target,
        row(pre_first),
        query_first,
        scratch=[pltpu.VMEM((rows, width), jnp.bfloat16)],
    )
    rim_target = shifted(tail, "sp", 1)
    across = swap(queries, "sp", 2)
    query_blocks = (queries, swap(queries, "sp", 1), across, swap(across, "sp", 1))

    span = source.shape[0] // CHUNKS
    beside = swap(source, "tp", 1)
    keyvals_first, keyvals_second = [], []
    for chunk in range(CHUNKS):
        cut = slice(chunk * span, (chunk + 1) * span)
        across = swap(source[cut], "tp", 2)
        chunk_rows, chunk_keyval = launch(
            functools.partial(keyval_body, cut),
            (shape_of(4 * span, width), shape_of(4 * span, keyval_width)),
            source,
            beside,
            across,
            swap(across, "tp", 1),
            row(source_gain),
            keyval_first,
        )
        keyvals_first.append(chunk_keyval)
        here = launch(project_body, shape_of(4 * span, keyval_width), chunk_rows, keyval_second)
        parts = [here]
        for bit in reversed(range((sp_count - 1).bit_length())):
            parts += [swap(part, "sp", 1 << bit) for part in parts]
        keyvals_second += parts

    packed = shape_of(rows + RIM_ROWS + STAT_ROWS, head_width)
    partials = [None] * sp_count
    for mask in range(sp_count):
        partial = launch(
            functools.partial(partial_body, mask, sp_count), packed, *query_blocks, *keyvals_first
        )
        partials[mask] = swap(partial, "sp", mask) if mask else partial

    def pair_sum(send, kept, weight):
        received = swap(send, "tp", 1)
        keep = launch(project_body, shape_of(*send.shape), kept, weight)
        return (keep.astype(jnp.float32) + received.astype(jnp.float32)).astype(jnp.bfloat16)

    def residual(own, post_gain, pre_gain, *streams):
        other = swap(own, "tp", 2)
        rims = tuple(shape_of(*stream.shape) for stream in streams[1:])
        return launch(
            residual_rim_body if rims else residual_body,
            (shape_of(half, width, jnp.float32), wide) + rims,
            own,
            other,
            *streams,
            row(post_gain),
            row(pre_gain),
        )

    send, kept = launch(
        join_send_body,
        (shape_of(half + RIM_ROWS, width), shape_of(half + RIM_ROWS, head_width)),
        *partials,
        out_first,
        scratch=[pltpu.VMEM((rows + RIM_ROWS, head_width), jnp.bfloat16)],
    )
    own = pair_sum(send, kept, out_first)
    after_first, hidden, rim = residual(own, post_first, ffn_pre, own_target, rim_target)
    send, kept = launch(
        mixer_body,
        (wide, shape_of(half, hidden_width)),
        hidden,
        swap(hidden, "tp", 1),
        rim,
        w_gate.T,
        w_value.T,
        conv_gate,
        conv_value,
        w_down,
        scratch=[pltpu.VMEM((rows + RIM_ROWS, hidden_width), jnp.float32)] * 2
        + [pltpu.VMEM((rows, hidden_width), jnp.bfloat16)],
    )
    own = pair_sum(send, kept, w_down)
    after_ffn, hidden = residual(own, ffn_post, pre_second, after_first)
    send, kept = launch(
        second_body,
        (wide, shape_of(half, head_width)),
        hidden,
        swap(hidden, "tp", 1),
        query_second,
        *keyvals_second,
        out_second,
        scratch=[pltpu.VMEM((rows, head_width), jnp.bfloat16)] * 2,
        limit=32,
    )
    own = pair_sum(send, kept, out_second)
    return launch(
        last_body,
        shape_of(quarter, width, jnp.float32),
        own[:quarter],
        swap(own[quarter:], "tp", 2),
        after_ffn[:quarter],
        row(post_second),
    )


def fits(mesh, target, query_first, keyval_first):
    blocks, places = mesh.shape["sp"], mesh.shape["tp"]
    return (
        places == len(LOCAL_ORDER)
        and blocks == 4
        and target.shape[0] == mesh.shape["grp"] * blocks * HEAD
        and keyval_first.shape[1] == 2 * HEAD * places
        and 3 * HEAD <= query_first.shape[1] // places <= STAT_ROWS * HEAD
    )


def solution(mesh):
    placed = (
        P(("grp", "sp", "tp"), None),
        P(("grp", "sp", "tp"), None),
        P(),
        P(),
        P(None, "tp"),
        P(None, "tp"),
        P("tp", None),
        P(),
        P(),
        P(None, "tp"),
        P(None, "tp"),
        P(None, "tp"),
        P(None, "tp"),
        P("tp", None),
        P(),
        P(),
        P(None, "tp"),
        P(None, "tp"),
        P("tp", None),
        P(),
    )
    placed_body = lambda body: jax.shard_map(
        body,
        mesh=mesh,
        in_specs=placed,
        out_specs=P(("grp", "sp", "tp"), None),
        check_vma=False,
    )


    def program(*arrays):
        if not fits(mesh, arrays[0], arrays[4], arrays[5]):
            return placed_body(per_device)(*arrays)
        return placed_body(per_device_paired)(*arrays)

    return program
```

```python
import functools

import jax
import jax.numpy as jnp
from jax import lax
from jax.experimental import pallas as pl
from jax.experimental.pallas import tpu as pltpu
from jax.sharding import PartitionSpec as P


HEAD = 128


def swapped(block, axis, distance):
    count = lax.axis_size(axis)
    route = []
    for low in range(count):
        high = low | 1 << distance
        if high != low and high < count:
            route += [(low, high), (high, low)]
    return lax.ppermute(block, axis, route)


def shifted(value, axis, steps):
    count = lax.axis_size(axis)
    leading, last = (max(0, -steps), min(count, count - steps))
    return lax.ppermute(value, axis, [(source, source + steps) for source in range(leading, last)])


def normed(values, gain):
    widened = values.astype(jnp.float32)
    return widened * lax.rsqrt(jnp.mean(widened * widened, axis=-1, keepdims=True) + 1e-06) * gain


def project_rows(rows_here, weights):
    shard_rows = lax.all_gather(rows_here, "tp", axis=0, tiled=True)
    products = [
        jnp.dot(shard_rows, weight, preferred_element_type=jnp.float32).astype(jnp.bfloat16)
        for weight in weights
    ]
    return jnp.concatenate(products, axis=1)


def summed_rows(parts, weight):
    return lax.psum_scatter(
        jnp.dot(parts, weight, preferred_element_type=jnp.float32).astype(jnp.bfloat16),
        "tp",
        scatter_dimension=0,
        tiled=True,
    ).astype(jnp.float32)


def key_columns(source_rows, keyval_first, keyval_second):
    both_layers = jnp.concatenate([keyval_first, keyval_second], axis=1)
    columns = jnp.einsum(
        "rd,dc->cr",
        lax.all_gather(source_rows, "tp", axis=0, tiled=True),
        both_layers,
        preferred_element_type=jnp.float32,
    ).astype(jnp.bfloat16)
    column_count = keyval_first.shape[1]
    stacked = columns.reshape(2, column_count, columns.shape[1])
    own_index = lax.axis_index("tp")
    doublings = (2 * HEAD // column_count).bit_length() - 1
    for bit_number in range(doublings):
        lower_half = own_index // 2**bit_number % 2 == 0
        outgoing = stacked
        retained = stacked
        partner = swapped(outgoing, "tp", bit_number)
        stacked = jnp.where(
            lower_half,
            jnp.concatenate([retained, partner], axis=1),
            jnp.concatenate([partner, retained], axis=1),
        )
    return (stacked[:, :HEAD], stacked[:, HEAD:])


def absorber(query_heads, running, shard_pair):
    scale_factor = HEAD ** (-0.5)
    best_score, weight_sum, weighted = running
    key_block, value_block = shard_pair
    scores = (
        jnp.einsum("thd,ds->ths", query_heads, key_block, preferred_element_type=jnp.float32)
        * scale_factor
    )
    newest = jnp.max(scores, axis=2)
    rescale = jnp.exp(best_score - newest)
    weights = jnp.exp(scores - newest[:, :, None])
    weight_sum = weight_sum * rescale + jnp.sum(weights, axis=2)
    weighted = weighted * rescale[:, :, None] + jnp.einsum(
        "ths,ds->thd", weights.astype(jnp.bfloat16), value_block, preferred_element_type=jnp.float32
    )
    return (newest, weight_sum, weighted)


def empty_running(row_count, head_count):
    return (
        jnp.full((row_count, head_count), -jnp.inf, jnp.float32),
        jnp.zeros((row_count, head_count), jnp.float32),
        jnp.zeros((row_count, head_count, HEAD), jnp.float32),
    )


def attend_keys(queries, keys_t, values_t):
    row_count = queries.shape[0]
    head_count = queries.shape[1] // HEAD
    query_heads = queries.reshape(row_count, head_count, HEAD)
    _, weight_sum, weighted = absorber(
        query_heads,
        empty_running(row_count, head_count),
        (
            lax.all_gather(keys_t, "sp", axis=1, tiled=True),
            lax.all_gather(values_t, "sp", axis=1, tiled=True),
        ),
    )
    return (
        (weighted / weight_sum[:, :, None])
        .reshape(row_count, head_count * HEAD)
        .astype(jnp.bfloat16)
    )


def causal_mix(rim_rows, up_rows, conv_taps):
    padded = jnp.concatenate([rim_rows, up_rows], axis=0).astype(jnp.float32)
    length = up_rows.shape[0]
    return (
        conv_taps[0] * padded[:length]
        + conv_taps[1] * padded[1 : length + 1]
        + conv_taps[2] * padded[2:]
    )


def per_device(
    target,
    source,
    source_gain,
    pre_first,
    query_first,
    keyval_first,
    out_first,
    post_first,
    ffn_pre,
    w_gate,
    w_value,
    conv_gate,
    conv_value,
    w_down,
    ffn_post,
    pre_second,
    query_second,
    keyval_second,
    out_second,
    post_second,
):
    source_rows = normed(source, source_gain).astype(jnp.bfloat16)
    keys_t, values_t = key_columns(source_rows, keyval_first, keyval_second)

    def attention_layer(stream, pre_gain, w_query, layer_index, w_out, post_gain):
        queries = project_rows(normed(stream, pre_gain).astype(jnp.bfloat16), (w_query,))
        heads = attend_keys(queries, keys_t[layer_index], values_t[layer_index])
        mixed = summed_rows(heads, w_out)
        return stream.astype(jnp.float32) + normed(mixed, post_gain)

    after_first = attention_layer(target, pre_first, query_first, 0, out_first, post_first)
    up_both = project_rows(normed(after_first, ffn_pre).astype(jnp.bfloat16), (w_gate, w_value))
    hidden_width = w_gate.shape[1]
    up_gate = up_both[:, :hidden_width]
    up_value = up_both[:, hidden_width:]
    rim_gate, rim_value = shifted((up_gate[-2:], up_value[-2:]), "sp", 1)
    gated = (
        jax.nn.gelu(causal_mix(rim_gate, up_gate, conv_gate), approximate=True)
        * causal_mix(rim_value, up_value, conv_value)
    ).astype(jnp.bfloat16)
    ffn_sum = summed_rows(gated, w_down)
    after_ffn = after_first + normed(ffn_sum, ffn_post)
    return attention_layer(after_ffn, pre_second, query_second, 1, out_second, post_second)


def swapped_mask(block, axis, mask):
    count = lax.axis_size(axis)
    return lax.ppermute(block, axis, [(index, index ^ mask) for index in range(count)])


def fetched(*arrays):
    count = len(arrays)

    def body(*refs):
        copies = [
            pltpu.make_async_copy(ref, out_ref, refs[-1].at[index])
            for index, (ref, out_ref) in enumerate(zip(refs[:count], refs[count:]))
        ]
        for copy in copies:
            copy.start()
        for copy in copies:
            copy.wait()

    return pl.pallas_call(
        body,
        out_shape=tuple(jax.ShapeDtypeStruct(array.shape, array.dtype) for array in arrays),
        in_specs=[pl.BlockSpec(memory_space=pl.ANY)] * count,
        scratch_shapes=[pltpu.SemaphoreType.DMA((count,))],
        compiler_params=pltpu.CompilerParams(vmem_limit_bytes=6 << 20),
    )(*arrays)


def launch(body, outs, *operands, scratch=(), limit=10):
    return pl.pallas_call(
        body,
        out_shape=outs,
        scratch_shapes=list(scratch),
        compiler_params=pltpu.CompilerParams(vmem_limit_bytes=limit << 20),
    )(*operands)


def dot32(left, right):
    return jnp.dot(left, right, preferred_element_type=jnp.float32)


LOCAL_ORDER = (0, 2, 1, 3)
RIM_ROWS = 8


def last_quarter():
    mask = lax.axis_index("tp") ^ 3
    return (mask >> 1) + (mask & 1) * 2


def tail_rows(ref, quarter):
    start = pl.multiple_of((last_quarter() + 1) * quarter - 2 * RIM_ROWS, 2 * RIM_ROWS)
    return ref[pl.ds(start, 2 * RIM_ROWS)][RIM_ROWS:]


def dot_nt(left, right):
    return lax.dot_general(
        left, right, (((1,), (1,)), ((), ())), preferred_element_type=jnp.float32
    )


def query_body(own_ref, other_ref, gain_ref, weight_ref, out_ref, rows_ref):
    half = own_ref.shape[0]
    for index, ref in enumerate((own_ref, other_ref)):
        here = slice(index * half, (index + 1) * half)
        rows_ref[here] = ref[...].astype(jnp.float32)
        hidden = normed(ref[...], gain_ref[...]).astype(jnp.bfloat16)
        out_ref[here] = dot32(hidden, weight_ref[...]).astype(jnp.bfloat16)
    width = out_ref.shape[1]
    tail = tail_rows(rows_ref, half // 2)
    out_ref[2 * half :] = jnp.concatenate(
        [
            tail[RIM_ROWS - 2 + index : RIM_ROWS - 1 + index, start : start + width]
            for index in range(2)
            for start in range(0, tail.shape[1], width)
        ],
        axis=0,
    ).astype(jnp.bfloat16)


def one_before(mask, block):
    return ((block ^ mask) - 1) ^ block


def chosen_part(parts, wanted):
    result = jnp.zeros(parts[0].shape, parts[0].dtype)
    for index, part in enumerate(parts):
        result = jnp.where(wanted == index, part, result)
    return result


def keyval_body(row_ref, gain_ref, mine_ref, theirs_ref, rows_out, mine_out, theirs_out):
    rows_out[...] = normed(row_ref[...], gain_ref[...]).astype(jnp.bfloat16)
    for weight_ref, out_ref in ((theirs_ref, theirs_out), (mine_ref, mine_out)):
        out_ref[...] = dot32(rows_out[...], weight_ref[...]).astype(jnp.bfloat16)


def keyval_later_body(*refs):
    *row_refs, mine_ref, theirs_ref, keyval_out, theirs_out = refs
    rows = jnp.concatenate([ref[...] for ref in row_refs], axis=0)
    for weight_ref, out_ref in ((theirs_ref, theirs_out), (mine_ref, keyval_out)):
        out_ref[...] = dot32(rows, weight_ref[...]).astype(jnp.bfloat16)


def turn_body(*refs):
    for ref, out_ref in zip(refs[: len(refs) // 2], refs[len(refs) // 2 :]):
        out_ref[...] = ref[...].T


def project_body(*refs):
    *row_refs, weight_ref, out_ref = refs
    start = 0
    for ref in row_refs:
        stop = start + ref.shape[0]
        out_ref[start:stop] = dot32(ref[...], weight_ref[...]).astype(jnp.bfloat16)
        start = stop


EXPONENT_SCALE = HEAD ** (-0.5) * 1.4426950408889634


def grouped(refs, size=4 * HEAD):
    groups, held = [], size
    for ref in refs:
        if held >= size:
            groups.append([])
            held = 0
        groups[-1].append(ref)
        held += ref.shape[0]
    return groups


def head_partial(query, keyval_refs):
    best = weighted = None
    for group in grouped(keyval_refs):
        keys, values = (
            jnp.concatenate([ref[:, cut] for ref in group], axis=0)
            for cut in (slice(None, HEAD), slice(HEAD, None))
        )
        scores = dot_nt(query, keys) * EXPONENT_SCALE
        newest = jnp.max(scores, axis=1, keepdims=True)
        if best is not None:
            newest = jnp.maximum(best, newest)
        weights = jnp.exp2(scores - newest).astype(jnp.bfloat16)
        added = dot32(weights, jnp.concatenate([values, jnp.ones_like(values)], axis=1))
        weighted = added if best is None else weighted * jnp.exp2(best - newest) + added
        best = newest
    return best, weighted[:, HEAD:], weighted[:, :HEAD]


def partial_body(mask, blocks, *refs):
    query_refs, keyval_refs, out_ref = refs[:blocks], refs[blocks:-1], refs[-1]
    rows, width = query_refs[0].shape[0] - RIM_ROWS, query_refs[0].shape[1]
    rim = chosen_part(
        [tail_rows(ref, rows // 4) for ref in query_refs], one_before(mask, lax.axis_index("sp"))
    )
    lane = lax.broadcasted_iota(jnp.int32, (rows + RIM_ROWS, HEAD), 1)
    levels = jnp.zeros((rows + RIM_ROWS, HEAD), jnp.float32)
    rim_parts = []
    for head in range(width // HEAD):
        columns = slice(head * HEAD, (head + 1) * HEAD)
        query = jnp.concatenate([query_refs[mask][:rows, columns], rim[:, columns]], axis=0)
        best, weight_sum, weighted = head_partial(query, keyval_refs)
        result = weighted / weight_sum
        out_ref[:rows, columns] = result[:rows].astype(jnp.bfloat16)
        rim_parts.append(result[rows:])
        levels = jnp.where(lane == head, best + jnp.log2(weight_sum), levels)
    left = levels[:rows].T[:RIM_ROWS]
    rim_left = jnp.concatenate([levels[rows + 2 :], levels[rows : rows + 2]], axis=0)
    row = lax.broadcasted_iota(jnp.int32, (RIM_ROWS, HEAD), 0)
    for piece in range(width // HEAD):
        here = jnp.where(row < 4, left, rim_left)
        here = jnp.where(row < RIM_ROWS - 2, here, rim_parts[piece]).astype(jnp.bfloat16)
        out_ref[rows:, piece * HEAD : (piece + 1) * HEAD] = here
        left = left - left.astype(jnp.bfloat16).astype(jnp.float32)
        rim_left = rim_left - rim_left.astype(jnp.bfloat16).astype(jnp.float32)


def shares_of(levels):
    best = functools.reduce(jnp.maximum, levels)
    shares = [jnp.exp2(level - best) for level in levels]
    total = functools.reduce(jnp.add, shares)
    return [share / total for share in shares]


def joined_heads(partial_refs, heads_ref):
    width = heads_ref.shape[1]
    rows = heads_ref.shape[0] - RIM_ROWS
    tails = [ref[rows:].astype(jnp.float32) for ref in partial_refs]
    levels = [sum(tail[:, piece * HEAD : (piece + 1) * HEAD] for piece in range(3)) for tail in tails]
    filler = jnp.zeros((HEAD - RIM_ROWS, rows), jnp.float32)
    columns = [jnp.concatenate([share, filler], axis=0).T for share in shares_of(levels)]
    rim_levels = [jnp.concatenate([level[-2:], level[:-2]], axis=0) for level in levels]
    for cut, parts in ((slice(0, rows), columns), (slice(rows, None), shares_of(rim_levels))):
        for head in range(width // HEAD):
            lanes = slice(head * HEAD, (head + 1) * HEAD)
            heads_ref[cut, lanes] = sum(
                ref[cut, lanes].astype(jnp.float32) * part[:, head : head + 1]
                for ref, part in zip(partial_refs, parts)
            ).astype(jnp.bfloat16)


def join_send_body(*refs):
    *partial_refs, weight_ref, send_ref, heads_out, heads_ref = refs
    joined_heads(partial_refs, heads_ref)
    half = (heads_ref.shape[0] - RIM_ROWS) // 2
    send_ref[...] = dot32(heads_ref[half:], weight_ref[...]).astype(jnp.bfloat16)
    heads_out[:half] = heads_ref[:half]
    heads_out[half:] = heads_ref[2 * half :]


def residual_body(own_ref, other_ref, *refs):
    stream_ref, post_ref, pre_ref, stream_out, hidden_out = refs
    half = stream_out.shape[0]
    quarter = half // 2
    for index in range(2):
        here = slice(index * quarter, (index + 1) * quarter)
        there = slice((1 - index) * quarter, (2 - index) * quarter)
        mixed = own_ref[here].astype(jnp.float32) + other_ref[there].astype(jnp.float32)
        stream = stream_ref[here].astype(jnp.float32) + normed(mixed, post_ref[...])
        stream_out[here] = stream
        hidden_out[here] = normed(stream, pre_ref[...]).astype(jnp.bfloat16)


def residual_rim_body(own_ref, other_ref, stream_ref, *refs):
    *query_refs, post_ref, pre_ref, stream_out, hidden_out, rim_out = refs
    residual_body(own_ref, other_ref, stream_ref, post_ref, pre_ref, stream_out, hidden_out)
    half = stream_out.shape[0]
    mixed = own_ref[half:].astype(jnp.float32) + other_ref[half:].astype(jnp.float32)
    rows = query_refs[0].shape[0] - RIM_ROWS
    wanted = one_before(0, lax.axis_index("sp"))
    packed = chosen_part([ref[rows:].astype(jnp.float32) for ref in query_refs], wanted)
    wide = RIM_ROWS // 2
    last_two = [
        jnp.concatenate([packed[row : row + 1] for row in range(index * wide, (index + 1) * wide)], axis=1)
        for index in range(2)
    ]
    rim_rows = jnp.concatenate(
        [jnp.zeros((RIM_ROWS - 2, mixed.shape[1]), jnp.float32), *last_two], axis=0
    )
    stream = rim_rows + normed(mixed, post_ref[...])
    rim = normed(stream, pre_ref[...])
    rim_out[...] = jnp.where(lax.axis_index("sp") == 0, 0.0, rim).astype(jnp.bfloat16)


def last_body(own_ref, other_ref, stream_ref, post_ref, out_ref):
    mixed = own_ref[...].astype(jnp.float32) + other_ref[...].astype(jnp.float32)
    out_ref[...] = stream_ref[...] + normed(mixed, post_ref[...])


def mixed_taps(ups, taps_ref):
    rows = ups.shape[0] - RIM_ROWS
    return sum(
        taps_ref[tap : tap + 1] * ups[RIM_ROWS - 2 + tap : RIM_ROWS - 2 + tap + rows].astype(jnp.float32)
        for tap in range(3)
    )


def mixer_body(
    own_ref,
    other_ref,
    rim_ref,
    gate_ref,
    value_ref,
    conv_gate,
    conv_value,
    down_ref,
    send_ref,
    gated_out,
    ups_gate,
    ups_value,
    gated_ref,
):
    quarter = own_ref.shape[0] // 2
    place = lax.axis_index("tp")
    starts = [pl.multiple_of((place ^ mask) * quarter, quarter) for mask in LOCAL_ORDER]
    rows = jnp.concatenate([own_ref[...], other_ref[...], rim_ref[...]], axis=0)
    for weight_ref, ups in ((gate_ref, ups_gate), (value_ref, ups_value)):
        product = dot32(rows, weight_ref[...])
        ups[:RIM_ROWS] = product[4 * quarter :].astype(jnp.bfloat16).astype(jnp.float32)
        for index, start in enumerate(starts):
            ups[pl.ds(start + RIM_ROWS, quarter)] = (
                product[index * quarter : (index + 1) * quarter].astype(jnp.bfloat16).astype(jnp.float32)
            )
    gated_ref[...] = (
        jax.nn.gelu(mixed_taps(ups_gate[...], conv_gate), approximate=True)
        * mixed_taps(ups_value[...], conv_value)
    ).astype(jnp.bfloat16)
    parts = [gated_ref[pl.ds(start, quarter)] for start in starts]
    send_ref[...] = dot32(jnp.concatenate(parts[2:], axis=0), down_ref[...]).astype(jnp.bfloat16)
    gated_out[...] = jnp.concatenate(parts[:2], axis=0)


def second_body(*refs):
    own_ref, other_ref, query_ref, *keyval_refs, weight_ref, send_ref, heads_out, queries_ref, heads_ref = refs
    half = own_ref.shape[0]
    queries_ref[:half] = dot32(own_ref[...], query_ref[...]).astype(jnp.bfloat16)
    queries_ref[half:] = dot32(other_ref[...], query_ref[...]).astype(jnp.bfloat16)
    for head in range(heads_ref.shape[1] // HEAD):
        columns = slice(head * HEAD, (head + 1) * HEAD)
        _, weight_sum, weighted = head_partial(queries_ref[:, columns], keyval_refs)
        heads_ref[:, columns] = (weighted / weight_sum).astype(jnp.bfloat16)
    send_ref[...] = dot32(heads_ref[half:], weight_ref[...]).astype(jnp.bfloat16)
    heads_out[...] = heads_ref[:half]


def shape_of(rows, columns, dtype=jnp.bfloat16):
    return jax.ShapeDtypeStruct((rows, columns), dtype)


CHUNKS = 2


def per_device_paired(
    target,
    source,
    source_gain,
    pre_first,
    query_first,
    keyval_first,
    out_first,
    post_first,
    ffn_pre,
    w_gate,
    w_value,
    conv_gate,
    conv_value,
    w_down,
    ffn_post,
    pre_second,
    query_second,
    keyval_second,
    out_second,
    post_second,
):
    quarter, width = target.shape
    half, rows = 2 * quarter, 4 * quarter
    head_width, keyval_width, hidden_width = query_first.shape[1], keyval_first.shape[1], w_gate.shape[1]
    sp_count = lax.axis_size("sp")
    row = lambda gain: gain.reshape(1, -1)
    swap = lambda value, axis, mask: swapped_mask(value, axis, mask)
    wide = shape_of(half, width)

    query_first, pre_first, source_gain = fetched(query_first, row(pre_first), row(source_gain))
    own_target = jnp.concatenate([target, swap(target, "tp", 2)], axis=0)
    other_target = swap(own_target, "tp", 1)
    queries = launch(
        query_body,
        shape_of(rows + RIM_ROWS, head_width),
        own_target,
        other_target,
        row(pre_first),
        query_first,
        scratch=[pltpu.VMEM((rows, width), jnp.float32)],
    )
    across = swap(queries, "sp", 2)
    query_blocks = (queries, swap(queries, "sp", 1), across, swap(across, "sp", 1))

    theirs = tuple(swap(weight, "tp", 1) for weight in (keyval_first, keyval_second))

    def keyvals_of(piece):
        size = piece.shape[0]
        normed_piece, mine, other = launch(
            keyval_body,
            (shape_of(size, width), shape_of(size, keyval_width), shape_of(size, keyval_width)),
            piece,
            row(source_gain),
            keyval_first,
            theirs[0],
        )
        return normed_piece, [mine, swap(other, "tp", 1)]

    def later_keyvals(*pieces):
        size = sum(piece.shape[0] for piece in pieces)
        mine, other = launch(
            keyval_later_body,
            (shape_of(size, keyval_width),) * 2,
            *pieces,
            keyval_second,
            theirs[1],
        )
        both = jnp.concatenate([mine, swap(other, "tp", 1)], axis=0)
        parts = [both]
        for bit in reversed(range((sp_count - 1).bit_length())):
            parts += [swap(block, "sp", 1 << bit) for block in parts]
        return parts

    span = source.shape[0] // CHUNKS
    normed_here, keyvals_first = keyvals_of(source)
    keyvals_second = later_keyvals(normed_here)
    normed_across = []
    for chunk in range(CHUNKS):
        across = swap(source[chunk * span : (chunk + 1) * span], "tp", 2)
        normed_piece, made = keyvals_of(across)
        normed_across.append(normed_piece)
        keyvals_first += made
    keyvals_second += later_keyvals(*normed_across)

    packed = shape_of(rows + RIM_ROWS, head_width)
    partials = [None] * sp_count
    for mask in range(sp_count):
        partial = launch(
            functools.partial(partial_body, mask, sp_count), packed, *query_blocks, *keyvals_first
        )
        partials[mask] = swap(partial, "sp", mask) if mask else partial

    def pair_sum(send, kept, weight):
        received = swap(send, "tp", 1)
        keep = launch(project_body, shape_of(*send.shape), kept, weight)
        return (keep.astype(jnp.float32) + received.astype(jnp.float32)).astype(jnp.bfloat16)

    def residual(own, post_gain, pre_gain, stream, *queries):
        other = swap(own, "tp", 2)
        return launch(
            residual_rim_body if queries else residual_body,
            (shape_of(half, width, jnp.float32), wide) + (shape_of(RIM_ROWS, width),) * bool(queries),
            own,
            other,
            stream,
            *queries,
            row(post_gain),
            row(pre_gain),
        )

    send, kept = launch(
        join_send_body,
        (shape_of(half + RIM_ROWS, width), shape_of(half + RIM_ROWS, head_width)),
        *partials,
        out_first,
        scratch=[pltpu.VMEM((rows + RIM_ROWS, head_width), jnp.bfloat16)],
    )
    own = pair_sum(send, kept, out_first)
    after_first, hidden, rim = residual(own, post_first, ffn_pre, own_target, *query_blocks)
    gate, value = launch(
        turn_body, (shape_of(width, hidden_width),) * 2, w_gate.T, w_value.T, limit=14
    )
    send, kept = launch(
        mixer_body,
        (wide, shape_of(half, hidden_width)),
        hidden,
        swap(hidden, "tp", 1),
        rim,
        gate,
        value,
        conv_gate,
        conv_value,
        w_down,
        scratch=[pltpu.VMEM((rows + RIM_ROWS, hidden_width), jnp.float32)] * 2
        + [pltpu.VMEM((rows, hidden_width), jnp.bfloat16)],
        limit=18,
    )
    own = pair_sum(send, kept, w_down)
    after_ffn, hidden = residual(own, ffn_post, pre_second, after_first)
    send, kept = launch(
        second_body,
        (wide, shape_of(half, head_width)),
        hidden,
        swap(hidden, "tp", 1),
        query_second,
        *keyvals_second,
        out_second,
        scratch=[pltpu.VMEM((rows, head_width), jnp.bfloat16)] * 2,
        limit=20,
    )
    own = pair_sum(send, kept, out_second)
    return launch(
        last_body,
        shape_of(quarter, width, jnp.float32),
        own[:quarter],
        swap(own[quarter:], "tp", 2),
        after_ffn[:quarter],
        row(post_second),
    )


def fits(mesh, target, source, query_first, keyval_first):
    blocks, places = mesh.shape["sp"], mesh.shape["tp"]
    return (
        places == len(LOCAL_ORDER)
        and blocks == 4
        and target.shape[0] == mesh.shape["grp"] * blocks * HEAD
        and source.shape[0] % (mesh.size * CHUNKS * HEAD) == 0
        and keyval_first.shape[1] == 2 * HEAD * places
        and query_first.shape[1] == 4 * HEAD * places
        and 2 * target.shape[1] == RIM_ROWS * query_first.shape[1] // places
    )


def solution(mesh):
    placed = (
        P(("grp", "sp", "tp"), None),
        P(("grp", "sp", "tp"), None),
        P(),
        P(),
        P(None, "tp"),
        P(None, "tp"),
        P("tp", None),
        P(),
        P(),
        P(None, "tp"),
        P(None, "tp"),
        P(None, "tp"),
        P(None, "tp"),
        P("tp", None),
        P(),
        P(),
        P(None, "tp"),
        P(None, "tp"),
        P("tp", None),
        P(),
    )
    placed_body = lambda body: jax.shard_map(
        body,
        mesh=mesh,
        in_specs=placed,
        out_specs=P(("grp", "sp", "tp"), None),
        check_vma=False,
    )


    def program(*arrays):
        if not fits(mesh, arrays[0], arrays[1], arrays[4], arrays[5]):
            return placed_body(per_device)(*arrays)
        return placed_body(per_device_paired)(*arrays)

    return program
```

```python
import functools

import jax
import jax.numpy as jnp
from jax import lax
from jax.experimental import pallas as pl
from jax.experimental.pallas import tpu as pltpu
from jax.sharding import PartitionSpec as P


HEAD = 128


def swapped(block, axis, distance):
    count = lax.axis_size(axis)
    route = []
    for low in range(count):
        high = low | 1 << distance
        if high != low and high < count:
            route += [(low, high), (high, low)]
    return lax.ppermute(block, axis, route)


def shifted(value, axis, steps):
    count = lax.axis_size(axis)
    leading, last = (max(0, -steps), min(count, count - steps))
    return lax.ppermute(value, axis, [(source, source + steps) for source in range(leading, last)])


def normed(values, gain):
    widened = values.astype(jnp.float32)
    return widened * lax.rsqrt(jnp.mean(widened * widened, axis=-1, keepdims=True) + 1e-06) * gain


def project_rows(rows_here, weights):
    shard_rows = lax.all_gather(rows_here, "tp", axis=0, tiled=True)
    products = [
        jnp.dot(shard_rows, weight, preferred_element_type=jnp.float32).astype(jnp.bfloat16)
        for weight in weights
    ]
    return jnp.concatenate(products, axis=1)


def summed_rows(parts, weight):
    return lax.psum_scatter(
        jnp.dot(parts, weight, preferred_element_type=jnp.float32).astype(jnp.bfloat16),
        "tp",
        scatter_dimension=0,
        tiled=True,
    ).astype(jnp.float32)


def key_columns(source_rows, keyval_first, keyval_second):
    both_layers = jnp.concatenate([keyval_first, keyval_second], axis=1)
    columns = jnp.einsum(
        "rd,dc->cr",
        lax.all_gather(source_rows, "tp", axis=0, tiled=True),
        both_layers,
        preferred_element_type=jnp.float32,
    ).astype(jnp.bfloat16)
    column_count = keyval_first.shape[1]
    stacked = columns.reshape(2, column_count, columns.shape[1])
    own_index = lax.axis_index("tp")
    doublings = (2 * HEAD // column_count).bit_length() - 1
    for bit_number in range(doublings):
        lower_half = own_index // 2**bit_number % 2 == 0
        outgoing = stacked
        retained = stacked
        partner = swapped(outgoing, "tp", bit_number)
        stacked = jnp.where(
            lower_half,
            jnp.concatenate([retained, partner], axis=1),
            jnp.concatenate([partner, retained], axis=1),
        )
    return (stacked[:, :HEAD], stacked[:, HEAD:])


def absorber(query_heads, running, shard_pair):
    scale_factor = HEAD ** (-0.5)
    best_score, weight_sum, weighted = running
    key_block, value_block = shard_pair
    scores = (
        jnp.einsum("thd,ds->ths", query_heads, key_block, preferred_element_type=jnp.float32)
        * scale_factor
    )
    newest = jnp.max(scores, axis=2)
    rescale = jnp.exp(best_score - newest)
    weights = jnp.exp(scores - newest[:, :, None])
    weight_sum = weight_sum * rescale + jnp.sum(weights, axis=2)
    weighted = weighted * rescale[:, :, None] + jnp.einsum(
        "ths,ds->thd", weights.astype(jnp.bfloat16), value_block, preferred_element_type=jnp.float32
    )
    return (newest, weight_sum, weighted)


def empty_running(row_count, head_count):
    return (
        jnp.full((row_count, head_count), -jnp.inf, jnp.float32),
        jnp.zeros((row_count, head_count), jnp.float32),
        jnp.zeros((row_count, head_count, HEAD), jnp.float32),
    )


def attend_keys(queries, keys_t, values_t):
    row_count = queries.shape[0]
    head_count = queries.shape[1] // HEAD
    query_heads = queries.reshape(row_count, head_count, HEAD)
    _, weight_sum, weighted = absorber(
        query_heads,
        empty_running(row_count, head_count),
        (
            lax.all_gather(keys_t, "sp", axis=1, tiled=True),
            lax.all_gather(values_t, "sp", axis=1, tiled=True),
        ),
    )
    return (
        (weighted / weight_sum[:, :, None])
        .reshape(row_count, head_count * HEAD)
        .astype(jnp.bfloat16)
    )


def causal_mix(rim_rows, up_rows, conv_taps):
    padded = jnp.concatenate([rim_rows, up_rows], axis=0).astype(jnp.float32)
    length = up_rows.shape[0]
    return (
        conv_taps[0] * padded[:length]
        + conv_taps[1] * padded[1 : length + 1]
        + conv_taps[2] * padded[2:]
    )


def per_device(
    target,
    source,
    source_gain,
    pre_first,
    query_first,
    keyval_first,
    out_first,
    post_first,
    ffn_pre,
    w_gate,
    w_value,
    conv_gate,
    conv_value,
    w_down,
    ffn_post,
    pre_second,
    query_second,
    keyval_second,
    out_second,
    post_second,
):
    source_rows = normed(source, source_gain).astype(jnp.bfloat16)
    keys_t, values_t = key_columns(source_rows, keyval_first, keyval_second)

    def attention_layer(stream, pre_gain, w_query, layer_index, w_out, post_gain):
        queries = project_rows(normed(stream, pre_gain).astype(jnp.bfloat16), (w_query,))
        heads = attend_keys(queries, keys_t[layer_index], values_t[layer_index])
        mixed = summed_rows(heads, w_out)
        return stream.astype(jnp.float32) + normed(mixed, post_gain)

    after_first = attention_layer(target, pre_first, query_first, 0, out_first, post_first)
    up_both = project_rows(normed(after_first, ffn_pre).astype(jnp.bfloat16), (w_gate, w_value))
    hidden_width = w_gate.shape[1]
    up_gate = up_both[:, :hidden_width]
    up_value = up_both[:, hidden_width:]
    rim_gate, rim_value = shifted((up_gate[-2:], up_value[-2:]), "sp", 1)
    gated = (
        jax.nn.gelu(causal_mix(rim_gate, up_gate, conv_gate), approximate=True)
        * causal_mix(rim_value, up_value, conv_value)
    ).astype(jnp.bfloat16)
    ffn_sum = summed_rows(gated, w_down)
    after_ffn = after_first + normed(ffn_sum, ffn_post)
    return attention_layer(after_ffn, pre_second, query_second, 1, out_second, post_second)


def swapped_mask(block, axis, mask):
    count = lax.axis_size(axis)
    return lax.ppermute(block, axis, [(index, index ^ mask) for index in range(count)])


def fetched(*arrays):
    count = len(arrays)

    def body(*refs):
        copies = [
            pltpu.make_async_copy(ref, out_ref, refs[-1].at[index])
            for index, (ref, out_ref) in enumerate(zip(refs[:count], refs[count:]))
        ]
        for copy in copies:
            copy.start()
        for copy in copies:
            copy.wait()

    return pl.pallas_call(
        body,
        out_shape=tuple(jax.ShapeDtypeStruct(array.shape, array.dtype) for array in arrays),
        in_specs=[pl.BlockSpec(memory_space=pl.ANY)] * count,
        scratch_shapes=[pltpu.SemaphoreType.DMA((count,))],
        compiler_params=pltpu.CompilerParams(vmem_limit_bytes=6 << 20),
    )(*arrays)


def launch(body, outs, *operands, scratch=(), limit=10):
    return pl.pallas_call(
        body,
        out_shape=outs,
        scratch_shapes=list(scratch),
        compiler_params=pltpu.CompilerParams(vmem_limit_bytes=limit << 20),
    )(*operands)


def dot32(left, right):
    return jnp.dot(left, right, preferred_element_type=jnp.float32)


LOCAL_ORDER = (0, 2, 1, 3)
RIM_ROWS = 8


def tail_rows(ref):
    rows = ref.shape[0] - RIM_ROWS
    return ref[rows - RIM_ROWS : rows]


def core_here():
    return lax.axis_index("tp") & 1


def half_rows(ref, core, half):
    return ref[pl.ds(pl.multiple_of(core * half, half), half)]


def dot_nt(left, right):
    return lax.dot_general(
        left, right, (((1,), (1,)), ((), ())), preferred_element_type=jnp.float32
    )


def query_body(own_ref, other_ref, gain_ref, weight_ref, out_ref, rows_ref):
    half = own_ref.shape[0]
    quarter = half // 2
    for index, mask in enumerate(LOCAL_ORDER):
        ref, start = (own_ref, other_ref)[index // 2], index % 2 * quarter
        place = pl.multiple_of((lax.axis_index("tp") ^ mask) * quarter, quarter)
        rows_ref[pl.ds(place, quarter)] = ref[start : start + quarter]
    hidden = normed(rows_ref[...], gain_ref[...]).astype(jnp.bfloat16)
    out_ref[: 2 * half] = dot32(hidden, weight_ref[...]).astype(jnp.bfloat16)
    width = out_ref.shape[1]
    tail = rows_ref[2 * half - RIM_ROWS :].astype(jnp.float32)
    out_ref[2 * half :] = jnp.concatenate(
        [
            tail[RIM_ROWS - 2 + index : RIM_ROWS - 1 + index, start : start + width]
            for index in range(2)
            for start in range(0, tail.shape[1], width)
        ],
        axis=0,
    ).astype(jnp.bfloat16)


def one_before(mask, block):
    return ((block ^ mask) - 1) ^ block


def chosen_part(parts, wanted):
    result = jnp.zeros(parts[0].shape, parts[0].dtype)
    for index, part in enumerate(parts):
        result = jnp.where(wanted == index, part, result)
    return result


def keyval_body(row_ref, gain_ref, mine_ref, theirs_ref, rows_out, mine_out, theirs_out):
    rows_out[...] = normed(row_ref[...], gain_ref[...]).astype(jnp.bfloat16)
    for weight_ref, out_ref in ((theirs_ref, theirs_out), (mine_ref, mine_out)):
        out_ref[...] = dot32(rows_out[...], weight_ref[...]).astype(jnp.bfloat16)


def keyval_later_body(*refs):
    *row_refs, mine_ref, theirs_ref, keyval_out, theirs_out = refs
    rows = jnp.concatenate([ref[...] for ref in row_refs], axis=0)
    for weight_ref, out_ref in ((theirs_ref, theirs_out), (mine_ref, keyval_out)):
        out_ref[...] = dot32(rows, weight_ref[...]).astype(jnp.bfloat16)


def turn_body(*refs):
    for ref, out_ref in zip(refs[: len(refs) // 2], refs[len(refs) // 2 :]):
        out_ref[...] = ref[...].T


def project_body(*refs):
    *row_refs, weight_ref, out_ref = refs
    start = 0
    for ref in row_refs:
        stop = start + ref.shape[0]
        out_ref[start:stop] = dot32(ref[...], weight_ref[...]).astype(jnp.bfloat16)
        start = stop


EXPONENT_SCALE = HEAD ** (-0.5) * 1.4426950408889634


def grouped(refs, size=4 * HEAD):
    groups, held = [], size
    for ref in refs:
        if held >= size:
            groups.append([])
            held = 0
        groups[-1].append(ref)
        held += ref.shape[0]
    return groups


def head_partial(query, keyval_refs, state=None):
    best, weighted = (None, None) if state is None else state
    for group in grouped(keyval_refs):
        keys, values = (
            jnp.concatenate([ref[:, cut] for ref in group], axis=0)
            for cut in (slice(None, HEAD), slice(HEAD, None))
        )
        scores = dot_nt(query, keys) * EXPONENT_SCALE
        newest = jnp.max(scores, axis=1, keepdims=True)
        if best is not None:
            newest = jnp.maximum(best, newest)
        weights = jnp.exp2(scores - newest).astype(jnp.bfloat16)
        added = dot32(weights, jnp.concatenate([values, jnp.ones_like(values)], axis=1))
        weighted = added if best is None else weighted * jnp.exp2(best - newest) + added
        best = newest
    return best, weighted[:, HEAD:], weighted[:, :HEAD]


def partial_body(mask, blocks, *refs):
    query_refs, keyval_refs, out_ref = refs[:blocks], refs[blocks:-1], refs[-1]
    rows, width = query_refs[0].shape[0] - RIM_ROWS, query_refs[0].shape[1]
    rim = chosen_part(
        [tail_rows(ref) for ref in query_refs], one_before(mask, lax.axis_index("sp"))
    )
    lane = lax.broadcasted_iota(jnp.int32, (rows + RIM_ROWS, HEAD), 1)
    levels = jnp.zeros((rows + RIM_ROWS, HEAD), jnp.float32)
    rim_parts = []
    for head in range(width // HEAD):
        columns = slice(head * HEAD, (head + 1) * HEAD)
        query = jnp.concatenate([query_refs[mask][:rows, columns], rim[:, columns]], axis=0)
        best, weight_sum, weighted = head_partial(query, keyval_refs)
        result = weighted / weight_sum
        out_ref[:rows, columns] = result[:rows].astype(jnp.bfloat16)
        rim_parts.append(result[rows:])
        levels = jnp.where(lane == head, best + jnp.log2(weight_sum), levels)
    left = levels[:rows].T[:RIM_ROWS]
    rim_left = jnp.concatenate([levels[rows + 2 :], levels[rows : rows + 2]], axis=0)
    row = lax.broadcasted_iota(jnp.int32, (RIM_ROWS, HEAD), 0)
    for piece in range(width // HEAD):
        here = jnp.where(row < 4, left, rim_left)
        here = jnp.where(row < RIM_ROWS - 2, here, rim_parts[piece]).astype(jnp.bfloat16)
        out_ref[rows:, piece * HEAD : (piece + 1) * HEAD] = here
        left = left - left.astype(jnp.bfloat16).astype(jnp.float32)
        rim_left = rim_left - rim_left.astype(jnp.bfloat16).astype(jnp.float32)


def shares_of(levels):
    best = functools.reduce(jnp.maximum, levels)
    shares = [jnp.exp2(level - best) for level in levels]
    total = functools.reduce(jnp.add, shares)
    return [share / total for share in shares]


def joined_heads(partial_refs, heads_ref):
    width = heads_ref.shape[1]
    rows = heads_ref.shape[0] - RIM_ROWS
    tails = [ref[rows:].astype(jnp.float32) for ref in partial_refs]
    levels = [sum(tail[:, piece * HEAD : (piece + 1) * HEAD] for piece in range(3)) for tail in tails]
    filler = jnp.zeros((HEAD - RIM_ROWS, rows), jnp.float32)
    columns = [jnp.concatenate([share, filler], axis=0).T for share in shares_of(levels)]
    rim_levels = [jnp.concatenate([level[-2:], level[:-2]], axis=0) for level in levels]
    for cut, parts in ((slice(0, rows), columns), (slice(rows, None), shares_of(rim_levels))):
        for head in range(width // HEAD):
            lanes = slice(head * HEAD, (head + 1) * HEAD)
            heads_ref[cut, lanes] = sum(
                ref[cut, lanes].astype(jnp.float32) * part[:, head : head + 1]
                for ref, part in zip(partial_refs, parts)
            ).astype(jnp.bfloat16)


def join_send_body(*refs):
    *partial_refs, weight_ref, send_ref, heads_out, heads_ref = refs
    joined_heads(partial_refs, heads_ref)
    half = (heads_ref.shape[0] - RIM_ROWS) // 2

    def rows_of(core):
        rim = jnp.where(core == 0, heads_ref[2 * half :], heads_ref[half - RIM_ROWS : half])
        return jnp.concatenate([half_rows(heads_ref, core, half), rim], axis=0)

    core = core_here()
    send_ref[...] = dot32(rows_of(1 - core), weight_ref[...]).astype(jnp.bfloat16)
    heads_out[...] = rows_of(core)


def residual_of(own_ref, other_ref, stream, post_ref, pre_ref):
    mixed = own_ref[...].astype(jnp.float32) + other_ref[...].astype(jnp.float32)
    stream = stream + normed(mixed, post_ref[...])
    return stream, normed(stream, pre_ref[...])


def first_residual_body(own_ref, other_ref, rows_ref, *refs):
    *query_refs, post_ref, pre_ref, stream_out, hidden_out, rim_out = refs
    half, core, block = stream_out.shape[0], core_here(), lax.axis_index("sp")
    rows = query_refs[0].shape[0] - RIM_ROWS
    packed = chosen_part([ref[rows:].astype(jnp.float32) for ref in query_refs], one_before(0, block))
    wide = RIM_ROWS // 2
    last_two = [
        jnp.concatenate([packed[row : row + 1] for row in range(index * wide, (index + 1) * wide)], axis=1)
        for index in range(2)
    ]
    before = jnp.concatenate(
        [jnp.zeros((RIM_ROWS - 2, rows_ref.shape[1]), jnp.float32), *last_two], axis=0
    )
    rim = jnp.where(core == 0, before, rows_ref[half - RIM_ROWS : half].astype(jnp.float32))
    stream = jnp.concatenate([half_rows(rows_ref, core, half).astype(jnp.float32), rim], axis=0)
    stream, hidden = residual_of(own_ref, other_ref, stream, post_ref, pre_ref)
    stream_out[...] = stream[:half]
    hidden_out[...] = hidden[:half].astype(jnp.bfloat16)
    edge = jnp.logical_and(core == 0, block == 0)
    rim_out[...] = jnp.where(edge, 0.0, hidden[half:]).astype(jnp.bfloat16)


def second_residual_body(own_ref, other_ref, stream_ref, post_ref, pre_ref, hidden_out, mine_out, give_out):
    stream, hidden = residual_of(own_ref, other_ref, stream_ref[...], post_ref, pre_ref)
    hidden_out[...] = hidden.astype(jnp.bfloat16)
    quarter = mine_out.shape[0]
    first, second = stream[:quarter], stream[quarter:]
    core = core_here()
    mine_out[...] = jnp.where(core == 0, first, second)
    give_out[...] = jnp.where(core == 0, second, first)


def last_body(own_ref, other_ref, mine_ref, given_ref, post_ref, out_ref):
    mixed = own_ref[...].astype(jnp.float32) + other_ref[...].astype(jnp.float32)
    here = lax.axis_index("tp") // 2 == core_here()
    out_ref[...] = jnp.where(here, mine_ref[...], given_ref[...]) + normed(mixed, post_ref[...])


def mixed_taps(ups, taps_ref):
    rows = ups.shape[0] - RIM_ROWS
    return sum(
        taps_ref[tap : tap + 1] * ups[RIM_ROWS - 2 + tap : RIM_ROWS - 2 + tap + rows].astype(jnp.float32)
        for tap in range(3)
    )


def mixer_body(own_ref, rim_ref, *refs):
    *half_refs, out_ref = refs
    rows = jnp.concatenate([rim_ref[...], own_ref[...]], axis=0)
    total = 0.0
    for gate_ref, value_ref, taps_ref, down_ref in (half_refs[:4], half_refs[4:]):
        taps = taps_ref[...]
        ups = [dot32(rows, ref[...]).astype(jnp.bfloat16).astype(jnp.float32) for ref in (gate_ref, value_ref)]
        gated = jax.nn.gelu(mixed_taps(ups[0], taps[:3]), approximate=True) * mixed_taps(ups[1], taps[3:])
        total += dot32(gated.astype(jnp.bfloat16), down_ref[...])
    out_ref[...] = total.astype(jnp.bfloat16)


STATE_WIDTH = 3 * HEAD


def second_early_body(*refs):
    own_ref, other_ref, query_ref, *keyval_refs, queries_ref, state_ref = refs
    half, core = own_ref.shape[0], core_here()
    for rows_ref, place in ((own_ref, core), (other_ref, 1 - core)):
        queries_ref[pl.ds(pl.multiple_of(place * half, half), half)] = dot32(
            rows_ref[...], query_ref[...]
        ).astype(jnp.bfloat16)
    for head in range(queries_ref.shape[1] // HEAD):
        columns = slice(head * HEAD, (head + 1) * HEAD)
        best, weight_sum, weighted = head_partial(queries_ref[:, columns], keyval_refs)
        held = (weighted, weight_sum, jnp.broadcast_to(best, weighted.shape))
        for place, part in enumerate(held):
            start = head * STATE_WIDTH + place * HEAD
            state_ref[:, start : start + HEAD] = part


def second_late_body(queries_ref, state_ref, keyval_ref, weight_ref, send_ref, heads_out, heads_ref):
    for head in range(heads_ref.shape[1] // HEAD):
        columns = slice(head * HEAD, (head + 1) * HEAD)
        start = head * STATE_WIDTH
        state = (
            state_ref[:, start + 2 * HEAD : start + 2 * HEAD + 1],
            state_ref[:, start : start + 2 * HEAD],
        )
        _, weight_sum, weighted = head_partial(queries_ref[:, columns], (keyval_ref,), state)
        heads_ref[:, columns] = (weighted / weight_sum).astype(jnp.bfloat16)
    quarter = heads_ref.shape[0] // 4
    parts = [
        heads_ref[pl.ds(pl.multiple_of((lax.axis_index("tp") ^ mask) * quarter, quarter), quarter)]
        for mask in LOCAL_ORDER
    ]
    send_ref[...] = dot32(jnp.concatenate(parts[2:], axis=0), weight_ref[...]).astype(jnp.bfloat16)
    heads_out[...] = jnp.concatenate(parts[:2], axis=0)


def shape_of(rows, columns, dtype=jnp.bfloat16):
    return jax.ShapeDtypeStruct((rows, columns), dtype)


CHUNKS = 2


def per_device_paired(
    target,
    source,
    source_gain,
    pre_first,
    query_first,
    keyval_first,
    out_first,
    post_first,
    ffn_pre,
    w_gate,
    w_value,
    conv_gate,
    conv_value,
    w_down,
    ffn_post,
    pre_second,
    query_second,
    keyval_second,
    out_second,
    post_second,
):
    quarter, width = target.shape
    half, rows = 2 * quarter, 4 * quarter
    head_width, keyval_width, hidden_width = query_first.shape[1], keyval_first.shape[1], w_gate.shape[1]
    sp_count = lax.axis_size("sp")
    row = lambda gain: gain.reshape(1, -1)
    swap = lambda value, axis, mask: swapped_mask(value, axis, mask)
    wide = shape_of(half, width)

    query_first, pre_first, source_gain = fetched(query_first, row(pre_first), row(source_gain))
    own_target = jnp.concatenate([target, swap(target, "tp", 2)], axis=0)
    other_target = swap(own_target, "tp", 1)
    queries, block_rows = launch(
        query_body,
        (shape_of(rows + RIM_ROWS, head_width), shape_of(rows, width)),
        own_target,
        other_target,
        row(pre_first),
        query_first,
    )
    across = swap(queries, "sp", 2)
    query_blocks = (queries, swap(queries, "sp", 1), across, swap(across, "sp", 1))

    theirs = tuple(swap(weight, "tp", 1) for weight in (keyval_first, keyval_second))

    def keyvals_of(piece):
        size = piece.shape[0]
        normed_piece, mine, other = launch(
            keyval_body,
            (shape_of(size, width), shape_of(size, keyval_width), shape_of(size, keyval_width)),
            piece,
            row(source_gain),
            keyval_first,
            theirs[0],
        )
        return normed_piece, [mine, swap(other, "tp", 1)]

    def later_keyvals(*pieces):
        size = sum(piece.shape[0] for piece in pieces)
        mine, other = launch(keyval_later_body, (shape_of(size, keyval_width),) * 2, *pieces, keyval_second, theirs[1])
        both = jnp.concatenate([mine, swap(other, "tp", 1)], axis=0)
        parts = [both]
        for bit in reversed(range((sp_count - 1).bit_length())):
            parts += [swap(block, "sp", 1 << bit) for block in parts]
        return parts

    bounds = (0, source.shape[0] * 3 // 4, source.shape[0])
    normed_here, keyvals_first = keyvals_of(source)
    keyvals_second = later_keyvals(normed_here)
    normed_across = []
    for chunk in range(CHUNKS):
        across = swap(source[bounds[chunk] : bounds[chunk + 1]], "tp", 2)
        normed_piece, made = keyvals_of(across)
        normed_across.append(normed_piece)
        keyvals_first += made
    keyvals_second += later_keyvals(*normed_across)

    packed = shape_of(rows + RIM_ROWS, head_width)
    partials = [None] * sp_count
    for mask in range(sp_count):
        partial = launch(functools.partial(partial_body, mask, sp_count), packed, *query_blocks, *keyvals_first)
        partials[mask] = swap(partial, "sp", mask) if mask else partial

    def pair_sum(send, kept, weight):
        received = swap(send, "tp", 1)
        keep = launch(project_body, shape_of(*send.shape), kept, weight)
        return (keep.astype(jnp.float32) + received.astype(jnp.float32)).astype(jnp.bfloat16)

    def residual(body, outs, own, post_gain, pre_gain, *streams):
        other = swap(own, "tp", 2)
        return launch(body, outs, own, other, *streams, row(post_gain), row(pre_gain))

    send, kept = launch(
        join_send_body,
        (shape_of(half + RIM_ROWS, width), shape_of(half + RIM_ROWS, head_width)),
        *partials,
        out_first,
        scratch=[pltpu.VMEM((rows + RIM_ROWS, head_width), jnp.bfloat16)],
    )
    own = pair_sum(send, kept, out_first)
    after_first, hidden, rim = residual(
        first_residual_body,
        (shape_of(half, width, jnp.float32), wide, shape_of(RIM_ROWS, width)),
        own,
        post_first,
        ffn_pre,
        block_rows,
        *query_blocks,
    )
    taps = jnp.concatenate([conv_gate, conv_value], axis=0)
    turned = launch(
        turn_body,
        (shape_of(width, hidden_width),) * 4,
        w_gate.T,
        w_value.T,
        swap(w_gate.T, "tp", 1),
        swap(w_value.T, "tp", 1),
        limit=24,
    )
    own = launch(
        mixer_body,
        wide,
        hidden,
        rim,
        *turned[:2],
        taps,
        w_down,
        *turned[2:],
        swap(taps, "tp", 1),
        swap(w_down, "tp", 1),
        limit=24,
    )
    quarter_shape = shape_of(quarter, width, jnp.float32)
    hidden, mine, give = residual(
        second_residual_body, (wide, quarter_shape, quarter_shape), own, ffn_post, pre_second, after_first
    )
    queries, state = launch(
        second_early_body,
        (shape_of(rows, head_width), shape_of(rows, head_width // HEAD * STATE_WIDTH, jnp.float32)),
        hidden,
        swap(hidden, "tp", 1),
        query_second,
        *keyvals_second[:-1],
        limit=20,
    )
    send, kept = launch(
        second_late_body,
        (wide, shape_of(half, head_width)),
        queries,
        state,
        keyvals_second[-1],
        out_second,
        scratch=[pltpu.VMEM((rows, head_width), jnp.bfloat16)],
    )
    own = pair_sum(send, kept, out_second)
    return launch(
        last_body,
        shape_of(quarter, width, jnp.float32),
        own[:quarter],
        swap(own[quarter:], "tp", 2),
        mine,
        swap(give, "tp", 1),
        row(post_second),
    )


def fits(mesh, target, source, query_first, keyval_first):
    blocks, places = mesh.shape["sp"], mesh.shape["tp"]
    return (
        places == len(LOCAL_ORDER)
        and blocks == 4
        and target.shape[0] == mesh.shape["grp"] * blocks * HEAD
        and source.shape[0] % (mesh.size * CHUNKS * HEAD) == 0
        and keyval_first.shape[1] == 2 * HEAD * places
        and query_first.shape[1] == 4 * HEAD * places
        and 2 * target.shape[1] == RIM_ROWS * query_first.shape[1] // places
    )


def solution(mesh):
    placed = (
        P(("grp", "sp", "tp"), None),
        P(("grp", "sp", "tp"), None),
        P(),
        P(),
        P(None, "tp"),
        P(None, "tp"),
        P("tp", None),
        P(),
        P(),
        P(None, "tp"),
        P(None, "tp"),
        P(None, "tp"),
        P(None, "tp"),
        P("tp", None),
        P(),
        P(),
        P(None, "tp"),
        P(None, "tp"),
        P("tp", None),
        P(),
    )
    placed_body = lambda body: jax.shard_map(
        body,
        mesh=mesh,
        in_specs=placed,
        out_specs=P(("grp", "sp", "tp"), None),
        check_vma=False,
    )


    def program(*arrays):
        if not fits(mesh, arrays[0], arrays[1], arrays[4], arrays[5]):
            return placed_body(per_device)(*arrays)
        return placed_body(per_device_paired)(*arrays)

    return program
```
